32 devices in a mesh: fs: 8 (over z, x), tp: 4 (over y, core).
Axes of the slice: x: 2, y: 2, z: 4, core: 2. Of those that a mesh axis runs over, the one named last changes fastest.
Arguments:
- later_input: bfloat16 [6144, 2048], P('fs', 'tp'), may hold values from -6 to 6
- earlier_input: bfloat16 [6144, 2048], P('fs', 'tp'), may hold values from -6 to 6
- cotangent: bfloat16 [6144, 2048], P('fs', 'tp'), may hold values from -6 to 6
- up_weight: bfloat16 [2048, 8192], P('fs', 'tp'), may hold values from -0.125 to 0.125
- down_weight: bfloat16 [8192, 2048], P('tp', 'fs'), may hold values from -0.0625 to 0.0625
- up_running: float32 [2048, 8192], P('fs', 'tp'), may hold values from -6 to 6
- down_running: float32 [2048, 8192], P('fs', 'tp'), may hold values from -6 to 6
Outputs:
- later_output: bfloat16 [6144, 2048], P('fs', 'tp')
- later_preact: bfloat16 [6144, 8192], P('fs', 'tp')
- earlier_grad: bfloat16 [6144, 2048], P('fs', 'tp')
- up_running_out: float32 [2048, 8192], P('fs', 'tp')
- down_running_out: float32 [2048, 8192], P('fs', 'tp')
The draws below stay inside these ranges and needn't reach their ends.
All inputs are finite; a program needn't handle non-finite values.
Results may differ from the reference program's by a relative error of at most 0.014.
Values may be sent and summed in bfloat16 or wider, within the bound.
A program may use at most 128 MiB of HBM per device.

```python
import jax
import jax.numpy as jnp
from jax import lax

D = 2048
FF = 8192
TOKENS = 6144
N_TP = 4


def with_spikes(values, own_key, source, target, blocks, factor):
    def block_of(axis_at):
        return (jnp.arange(values.shape[axis_at]) // (values.shape[axis_at] // blocks)).reshape((-1,) + (1,) * (values.ndim - 1 - axis_at))

    near = jax.random.permutation(own_key, blocks)[block_of(target)]
    far = (block_of(target) + blocks // 2) % blocks
    return jnp.where((block_of(source) == near) | (block_of(source) == far), factor * values, values)


def steps_of(rng, shape, pieces, least, top_value):
    factor_of, own = 1.0, jax.random.fold_in(rng, 6)
    for position, blocks in pieces:
        steps = jnp.exp(jax.random.uniform(jax.random.fold_in(own, position), (blocks,), jnp.float32, least / len(pieces), top_value / len(pieces)))
        factor_of = factor_of * jnp.repeat(steps, shape[position] // blocks).reshape([-1 if axis == position else 1 for axis in range(len(shape))])
    return factor_of


def scatter_about(key, dims, scale, bound, split=(), kind=jnp.bfloat16):
    result = scale * jax.random.normal(key, dims, jnp.float32)
    if split:
        result = result * steps_of(key, dims, split, -0.22, 0.18)
    return jnp.clip(result, -bound, bound).astype(kind)


def heavy_noise(own_key, dims, scale, reach, split, heavy, held_as=jnp.bfloat16):
    drawn = scale * jax.random.normal(own_key, dims, jnp.float32)
    if split:
        drawn = drawn * steps_of(own_key, dims, split, -0.22, 0.18)
    return jnp.clip(with_spikes(drawn, jax.random.fold_in(own_key, 3), *heavy), -reach, reach).astype(held_as)


def setup_inputs(seed: int = 0) -> dict:
    splits = jax.random.split(jax.random.key(seed), 8)
    return {
        "later_input": scatter_about(splits[0], (TOKENS, D), 1.0, 6.0, ((0, 8), (1, 4))),
        "earlier_input": scatter_about(splits[1], (TOKENS, D), 1.0, 6.0, ((0, 8), (1, 4))),
        "cotangent": heavy_noise(splits[2], (TOKENS, D), 1.0, 6.0, ((0, 8), (1, 4)), (0, 1, 8, 2.0)),
        "up_weight": scatter_about(splits[3], (D, FF), D ** -0.5, 0.125, ((0, 8), (1, 4))),
        "down_weight": scatter_about(splits[4], (FF, D), FF ** -0.5, 0.0625, ((0, 4), (1, 8))),
        "up_running": scatter_about(splits[5], (D, FF), 1.0, 6.0, ((0, 8), (1, 4)), jnp.float32),
        "down_running": scatter_about(splits[6], (D, FF), 1.0, 6.0, ((0, 8), (1, 4)), jnp.float32),
    }


def block_sum(left, right):
    rows = left.shape[0]
    width = left.shape[1] // N_TP
    left_blocks = left.reshape(rows, N_TP, width).transpose(1, 0, 2)
    right_blocks = right.reshape(N_TP, width, right.shape[1])

    def step(total, pair):
        part = jnp.dot(pair[0], pair[1], preferred_element_type=jnp.float32).astype(jnp.bfloat16)
        part = lax.optimization_barrier(part)
        return total + part.astype(jnp.float32), None

    start = jnp.zeros((rows, right.shape[1]), jnp.float32)
    total, _ = lax.scan(step, start, (left_blocks, right_blocks))
    return total.astype(jnp.bfloat16)


def reference(later_input, earlier_input, cotangent, up_weight, down_weight, up_running, down_running):
    later_up = jnp.dot(later_input, up_weight, preferred_element_type=jnp.float32)
    later_preact = later_up.astype(jnp.bfloat16)
    later_hidden = jnp.square(jax.nn.relu(later_up)).astype(jnp.bfloat16)
    later_output = block_sum(later_hidden, down_weight)
    earlier_up = jnp.dot(earlier_input, up_weight, preferred_element_type=jnp.float32)
    earlier_hidden = jnp.square(jax.nn.relu(earlier_up)).astype(jnp.bfloat16)
    hidden_grad = jnp.dot(cotangent, down_weight.T, preferred_element_type=jnp.float32)
    up_grad = (2.0 * jax.nn.relu(earlier_up) * hidden_grad).astype(jnp.bfloat16)
    earlier_grad = block_sum(up_grad, up_weight.T)
    factor = float(TOKENS) ** -0.5
    up_running_out = up_running + jnp.dot(earlier_input.T, up_grad, preferred_element_type=jnp.float32) * factor
    down_running_out = down_running + jnp.dot(cotangent.T, earlier_hidden, preferred_element_type=jnp.float32) * factor
    return later_output, later_preact, earlier_grad, up_running_out, down_running_out
```

```python
import functools
import math

import jax
import jax.numpy as jnp
from jax import lax
from jax.experimental import pallas as pl
from jax.experimental.pallas import tpu as pltpu
from jax.sharding import PartitionSpec as P

contract_last = (((1,), (1,)), ((), ()))
contract_first = (((0,), (0,)), ((), ()))


STREAMS = 4


def ring_index(place, n):
    place = lax.rem(place + 2 * n, n)
    return jnp.where(place < n // 2, 2 * place, 2 * (n - place) - 1)


def ring_pairs(n, direction):
    order = [q * 2 if q < n // 2 else 2 * (n - q) - 1 for q in range(n)]
    return [(order[q], order[(q + direction) % n]) for q in range(n)]


def my_place(n):
    me = lax.axis_index("fs")
    half = lax.div(me, 2)
    return jnp.where(lax.rem(me, 2) == 0, half, n - 1 - half)


def after(value, *others):
    return lax.optimization_barrier((value, *others))[0]


def ring_gather(shard):
    n = lax.axis_size("fs")
    rows, columns = shard.shape
    place = my_place(n)
    blocks = shard.reshape(STREAMS, rows // STREAMS, columns)
    held = [blocks[s : s + 1] for s in range(STREAMS)]
    full = jnp.zeros((n, STREAMS, rows // STREAMS, columns), shard.dtype)
    full = lax.dynamic_update_slice(full, blocks[None], (lax.axis_index("fs"), 0, 0, 0))
    arrived = []
    for step in range(1, n):
        for s in range(STREAMS):
            direction = 1 if s % 2 == 0 else -1
            held[s] = lax.ppermute(held[s], "fs", ring_pairs(n, direction))
            owner = ring_index(place - direction * step, n)
            full = lax.dynamic_update_slice(full, held[s][None], (owner, s, 0, 0))
        arrived.append(tuple(held))
    return full.reshape(n * rows, columns), arrived


def ring_scatter(terms, wait_for=()):
    n = lax.axis_size("fs")
    rows, columns = terms.shape[0] // n, terms.shape[1]
    place = my_place(n)
    blocks = terms.reshape(n, STREAMS, rows // STREAMS, columns)

    def own(s, direction, step):
        owner = ring_index(place - direction * (step + 1), n)
        return lax.dynamic_slice(
            blocks, (owner, s, 0, 0), (1, 1, rows // STREAMS, columns)
        ).reshape(rows // STREAMS, columns)

    totals = [own(s, 1 if s % 2 == 0 else -1, 0) for s in range(STREAMS)]
    if wait_for:
        totals = [after(total, *wait_for) for total in totals]
    for step in range(1, n):
        for s in range(STREAMS):
            direction = 1 if s % 2 == 0 else -1
            got = lax.ppermute(
                totals[s].astype(jnp.bfloat16), "fs", ring_pairs(n, direction)
            )
            totals[s] = got.astype(jnp.float32) + own(s, direction, step).astype(jnp.float32)
    return jnp.concatenate(totals, axis=0)


def flip_pairs(n, mask):
    return [(i, i ^ mask) for i in range(n)]


def tp_gather(block):
    n = lax.axis_size("tp")
    me = lax.axis_index("tp")
    blocks = [block]
    mask = n // 2
    while mask:
        upper = (me & mask) != 0
        merged = []
        for mine in blocks:
            other = lax.ppermute(mine, "tp", flip_pairs(n, mask))
            merged += [jnp.where(upper, other, mine), jnp.where(upper, mine, other)]
        blocks = merged
        mask //= 2
    return jnp.concatenate(blocks, axis=-1)


def tp_scatter(terms):
    n = lax.axis_size("tp")
    me = lax.axis_index("tp")
    width = terms.shape[1] // n
    blocks = [terms[:, j * width : (j + 1) * width] for j in range(n)]
    mask = 1
    while mask < n:
        upper = (me & mask) != 0
        kept = []
        for low, high in zip(blocks[0::2], blocks[1::2]):
            sent = jnp.where(upper, low, high).astype(jnp.bfloat16)
            mine = jnp.where(upper, high, low)
            got = lax.ppermute(sent, "tp", flip_pairs(n, mask))
            kept.append(mine.astype(jnp.float32) + got.astype(jnp.float32))
        blocks = kept
        mask *= 2
    return blocks[0].astype(jnp.bfloat16)


MESH = pl.DeviceIdType.MESH
VMEM_BYTES = 67043328


def span(start, size):
    if not isinstance(start, int):
        start = pl.multiple_of(start, size)
    return pl.ds(start, size)


def layer_kernel(
    nz,
    later_in,
    earlier_in,
    cot_in,
    up_in,
    down_in,
    later_out,
    preact_out,
    grad_out,
    up_out,
    down_out,
    later_x,
    earlier_x,
    cot_x,
    up_w,
    down_w,
    gate,
    hidden,
    squared,
    staged,
    down_terms,
    up_terms,
    down_got,
    up_got,
    parts_got,
    last_got,
    send_sem,
    recv_sem,
    local_sem,
    ready_sem,
):
    fs, tp = lax.axis_index("fs"), lax.axis_index("tp")
    z, x = lax.div(fs, 2), lax.rem(fs, 2)
    y, k = lax.div(tp, 2), lax.rem(tp, 2)
    ox, oy, ok = 1 - x, 1 - y, 1 - k
    at_x, at_y, at_k = (z * 2 + ox, tp), (fs, oy * 2 + k), (fs, y * 2 + ok)
    at_up, at_down = (fs + 2, tp), (fs - 2, tp)
    top = nz - 1

    tokens, feats = later_in.shape
    fan = up_in.shape[0]
    width = up_w.shape[1]
    slab = 2 * fan
    chunks = 2
    cw = width // chunks
    tile = math.gcd(tokens, slab)

    ids = {}
    pending = []

    def sid(name, count=1):
        if name not in ids:
            ids[name] = sum(c for _, c in ids.values()), count
        return ids[name][0]

    def remote(src, dst, index, device):
        return pltpu.make_async_remote_copy(
            src_ref=src,
            dst_ref=dst,
            send_sem=send_sem.at[index],
            recv_sem=recv_sem.at[index],
            device_id=device,
            device_id_type=MESH,
        )

    def send(src, dst, index, device, when=None):
        def go():
            remote(src(), dst(), index, device).start()

        if when is None:
            go()
        else:
            pl.when(when)(go)
        pending.append((src, dst, index, device, when))

    def sent(entry):
        src, dst, index, device, when = entry

        def go():
            remote(src(), dst(), index, device).wait_send()

        if when is None:
            go()
        else:
            pl.when(when)(go)

    def drain(start, stop):
        for entry in pending[start:stop]:
            sent(entry)

    def arrived(dst, index):
        remote(dst, dst, index, at_x).wait_recv()

    barrier = pltpu.get_barrier_semaphore()
    for device in (at_x, at_y, at_k):
        pl.semaphore_signal(barrier, inc=1, device_id=device, device_id_type=MESH)

    @pl.when(z > 0)
    def _():
        pl.semaphore_signal(barrier, inc=1, device_id=at_down, device_id_type=MESH)

    @pl.when(z < top)
    def _():
        pl.semaphore_signal(barrier, inc=1, device_id=at_up, device_id_type=MESH)

    pl.semaphore_wait(barrier, 3 + jnp.where(z > 0, 1, 0) + jnp.where(z < top, 1, 0))

    def block(ref, xx, yy, kk):
        return ref.at[span(xx * tokens, tokens), span((yy * 2 + kk) * feats, feats)]

    def up_block(zz, xx):
        return up_w.at[span((zz * 2 + xx) * fan, fan), :]

    def down_block(zz, xx):
        return down_w.at[:, span((zz * 2 + xx) * fan, fan)]

    def line_first(name, own, place, xx):
        base = sid(name, 2 * nz)
        send(own, lambda: place(z, xx), base, at_up, z < top)
        send(own, lambda: place(z, xx), base + nz, at_down, z > 0)

    def line_hop(name, place, xx, hop):
        base = sid(name, 2 * nz)

        @pl.when(z >= hop)
        def _():
            arrived(place(z - hop, xx), base + hop - 1)

        if hop < top:
            here = lambda: place(z - hop, xx)
            send(here, here, base + hop, at_up, (z >= hop) & (z < top))

        @pl.when(z + hop <= top)
        def _():
            arrived(place(z + hop, xx), base + nz + hop - 1)

        if hop < top:
            here = lambda: place(z + hop, xx)
            send(here, here, base + nz + hop, at_down, (z + hop <= top) & (z > 0))

    class Rows:
        def __init__(self, name, own, full):
            self.name, self.own, self.full = name, own, full
            self.copy = pltpu.make_async_copy(own, block(full, x, y, k), local_sem.at[sid("local " + name)])

        def local(self):
            self.copy.start()

        def to(self, way, source, xx, yy, device):
            here = lambda: block(self.full, xx, yy, k)
            send((lambda: self.own) if source else here, here, sid(self.name + way), device)

        def first_x(self):
            self.to("x", True, x, y, at_x)

        def first_y(self):
            self.to("y", True, x, y, at_y)

        def first_k(self):
            self.to("k0", True, x, y, at_k)

        def got_x(self):
            arrived(block(self.full, ox, y, k), sid(self.name + "x"))
            self.to("xy", False, ox, y, at_y)
            self.to("k1", False, ox, y, at_k)

        def got_y(self):
            arrived(block(self.full, x, oy, k), sid(self.name + "y"))
            self.to("k2", False, x, oy, at_k)

        def got_xy(self):
            arrived(block(self.full, ox, oy, k), sid(self.name + "xy"))
            self.to("k3", False, ox, oy, at_k)

        def whole(self):
            self.copy.wait()
            for way, xx, yy in (("k0", x, y), ("k1", ox, y), ("k2", x, oy), ("k3", ox, oy)):
                arrived(block(self.full, xx, yy, ok), sid(self.name + way))

    ex = Rows("ex", earlier_in, earlier_x)
    ct = Rows("ct", cot_in, cot_x)
    lx = Rows("lx", later_in, later_x)
    up_own = up_in.at[:, span(x * width, width)]
    up_other = up_in.at[:, span(ox * width, width)]
    down_own = down_in.at[span(x * width, width), :]
    down_other = down_in.at[span(ox * width, width), :]
    up_copy = pltpu.make_async_copy(up_own, up_block(z, x), local_sem.at[sid("local up")])
    down_copy = pltpu.make_async_copy(down_own, down_block(z, x), local_sem.at[sid("local down")])

    line_first("uA", lambda: up_own, up_block, x)
    ex.first_x()
    ex.first_y()
    send(lambda: up_other, lambda: up_block(z, x), sid("ux"), at_x)
    ct.first_x()
    ct.first_y()
    ex.first_k()
    ct.first_k()
    up_copy.start()
    ex.local()
    ct.local()
    lx.local()
    down_copy.start()
    send(lambda: down_other, lambda: down_block(z, x), sid("dx"), at_x)
    lx.first_x()
    lx.first_k()

    line_hop("uA", up_block, x, 1)
    ex.got_x()
    ex.got_y()
    line_hop("uA", up_block, x, 2)
    arrived(up_block(z, ox), sid("ux"))
    line_first("uB", lambda: up_block(z, ox), up_block, ox)
    line_hop("uA", up_block, x, 3)
    ct.got_y()
    line_hop("uB", up_block, ox, 1)
    ct.got_x()
    lx.first_y()
    ex.got_xy()
    line_hop("uB", up_block, ox, 2)
    line_first("dA", lambda: down_own, down_block, x)
    arrived(down_block(z, ox), sid("dx"))
    up_copy.wait()
    line_hop("uB", up_block, ox, 3)
    ex.whole()

    def dot(a, b, dims):
        return lax.dot_general(a, b, (dims, ((), ())), preferred_element_type=jnp.float32)

    row_tiles = 2 * tokens // tile

    def gate_chunk(j):
        @pl.loop(0, row_tiles)
        def _(i):
            rows, cols = span(i * tile, tile), span(j * cw, cw)
            value = jnp.maximum(dot(earlier_x[rows, :], up_w[:, cols], ((1,), (0,))), 0.0)
            gate[rows, cols] = value.astype(jnp.bfloat16)
            squared[rows, :] = (value * value).astype(jnp.bfloat16)

    def later_chunk(j, place):
        cols = span(j * cw, cw)

        @pl.loop(0, row_tiles)
        def _(i):
            rows = span(i * tile, tile)
            value = dot(later_x[rows, :], up_w[:, cols], ((1,), (0,)))
            place[rows, :] = value.astype(jnp.bfloat16)
            value = jnp.maximum(value, 0.0)
            hidden[rows, cols] = (value * value).astype(jnp.bfloat16)

        out_cols = span(x * width + j * cw, cw)
        send(
            lambda: place.at[span(ox * tokens, tokens), :],
            lambda: preact_out.at[:, out_cols],
            sid(f"pre{j}"),
            at_x,
        )
        copy = pltpu.make_async_copy(
            place.at[span(x * tokens, tokens), :],
            preact_out.at[:, out_cols],
            local_sem.at[sid(f"local pre{j}")],
        )
        copy.start()
        return copy

    def slope_chunk(j):
        @pl.loop(0, row_tiles)
        def _(i):
            rows, cols = span(i * tile, tile), span(j * cw, cw)
            value = dot(cot_x[rows, :], down_w[cols, :], ((1,), (1,)))
            value = 2.0 * gate[rows, cols].astype(jnp.float32) * value
            gate[rows, cols] = value.astype(jnp.bfloat16)

    class Sum:
        def __init__(self, name, left, terms, got, out):
            self.name, self.left, self.terms, self.got, self.out = name, left, terms, got, out

        def part(self, o, j):
            return self.terms.at[span(o * slab, slab), span(j * cw, cw)]

        def slot(self, s, j):
            return self.got.at[s, :, span(j * cw, cw)]

        def compute(self, j, right):
            base = sid(f"{self.name}{j}", 2 * nz)
            for s in range(nz):
                o = jnp.where(z * 2 < nz, top - s, s)

                @pl.loop(0, slab // tile)
                def _(i):
                    rows = span(o * slab + i * tile, tile)
                    value = dot(self.left[:, rows], right(), ((0,), (0,)))
                    self.terms[rows, span(j * cw, cw)] = value.astype(jnp.bfloat16)

                if s < top:
                    up, down = top - s, s
                    send(
                        lambda up=up: self.part(up, j),
                        lambda up=up: self.slot(up + 1, j),
                        base + up,
                        at_up,
                        z == 0,
                    )
                    send(
                        lambda down=down: self.part(down, j),
                        lambda down=down: self.slot(down, j),
                        base + nz + down,
                        at_down,
                        z == top,
                    )

        def add(self, o, s, j):
            @pl.loop(0, slab // tile)
            def _(i):
                rows, cols = span(o * slab + i * tile, tile), span(j * cw, cw)
                value = self.terms[rows, cols].astype(jnp.float32)
                value = value + self.got[s, span(i * tile, tile), cols].astype(jnp.float32)
                self.terms[rows, cols] = value.astype(jnp.bfloat16)

        def step(self, t, j):
            base = sid(f"{self.name}{j}", 2 * nz)
            up = top - t + z
            down = z - (top - t)

            @pl.when((z >= 1) & (t >= z))
            def _():
                arrived(self.slot(up + 1, j), base + up)
                self.add(up, up + 1, j)

            if t < top:
                send(
                    lambda: self.part(up, j),
                    lambda: self.slot(up + 1, j),
                    base + up,
                    at_up,
                    (z >= 1) & (t >= z),
                )

            @pl.when((z < top) & (t >= top - z))
            def _():
                arrived(self.slot(down, j), base + nz + down)
                self.add(down, down, j)

            if t < top:
                send(
                    lambda: self.part(down, j),
                    lambda: self.slot(down, j),
                    base + nz + down,
                    at_down,
                    (z < top) & (t >= top - z),
                )
            else:
                rows = lambda xx: span(z * slab + xx * fan, fan)
                cols, out_cols = span(j * cw, cw), span(x * width + j * cw, cw)
                send(
                    lambda: self.terms.at[rows(ox), cols],
                    lambda: self.out.at[:, out_cols],
                    sid(f"{self.name}x{j}"),
                    at_x,
                )
                copy = pltpu.make_async_copy(
                    self.terms.at[rows(x), cols],
                    self.out.at[:, out_cols],
                    local_sem.at[sid(f"local {self.name}{j}")],
                )
                copy.start()
                locals_.append(copy)

        def finish(self):
            for j in range(chunks):
                arrived(
                    self.out.at[:, span(ox * width + j * cw, cw)], sid(f"{self.name}x{j}")
                )

    class Partial:
        def __init__(self, name, left, right, dims, total, got, last, out):
            self.name, self.left, self.right, self.dims = name, left, right, dims
            self.total, self.got, self.last, self.out = total, got, last, out

        def rows(self, h):
            return ox if h == 0 else x

        def tile_of(self, h, yy, kk):
            return self.total.at[
                span(self.rows(h) * tokens, tokens), span((yy * 2 + kk) * feats, feats)
            ]

        def slot(self, h, c):
            return self.got.at[span(h * tokens, tokens), span(c * feats, feats)]

        def columns(self, h, kk):
            for yy in range(2):
                cols = span((yy * 2 + kk) * feats, feats)

                @pl.loop(0, tokens // tile)
                def _(i):
                    rows = span(self.rows(h) * tokens + i * tile, tile)
                    right = self.right[cols, :] if self.dims == ((1,), (1,)) else self.right[:, cols]
                    value = dot(self.left[rows, :], right, self.dims)
                    self.total[rows, cols] = value.astype(jnp.bfloat16)

        def compute(self, h):
            self.columns(h, ok)
            for yy in range(2):
                send(
                    lambda yy=yy: self.tile_of(h, yy, ok),
                    lambda yy=yy: self.slot(h, yy),
                    sid(f"{self.name}k{h}{yy}"),
                    at_k,
                )
            self.columns(h, k)

        def add(self, h, yy, got):
            mine = self.tile_of(h, yy, k)

            @pl.loop(0, tokens // tile)
            def _(i):
                rows = span(i * tile, tile)
                value = mine[rows, :].astype(jnp.float32) + got[rows, :].astype(jnp.float32)
                mine[rows, :] = value.astype(jnp.bfloat16)

        def after_k(self, h):
            for yy in range(2):
                arrived(self.slot(h, yy), sid(f"{self.name}k{h}{yy}"))
            self.add(h, oy, self.got.at[span(h * tokens, tokens), span(oy * feats, feats)])
            send(
                lambda: self.tile_of(h, oy, k),
                lambda: self.slot(h, 2),
                sid(f"{self.name}y{h}"),
                at_y,
            )
            self.add(h, y, self.got.at[span(h * tokens, tokens), span(y * feats, feats)])

        def after_y(self, h):
            arrived(self.slot(h, 2), sid(f"{self.name}y{h}"))
            self.add(h, y, self.slot(h, 2))
            if h == 0:
                send(
                    lambda: self.tile_of(0, y, k),
                    lambda: self.last,
                    sid(f"{self.name}x"),
                    at_x,
                )

        def finish(self):
            arrived(self.last, sid(f"{self.name}x"))
            self.add(1, y, self.last)
            copy = pltpu.make_async_copy(
                self.tile_of(1, y, k), self.out, local_sem.at[sid(f"local {self.name}")]
            )
            copy.start()
            locals_.append(copy)

    locals_ = []
    down_sum = Sum("ds", cot_x, down_terms, down_got, down_out)
    up_sum = Sum("us", earlier_x, up_terms, up_got, up_out)
    cols_of = lambda j: span(j * cw, cw)

    gate_chunk(0)
    ct.got_xy()
    ct.whole()
    down_sum.compute(0, lambda: squared[...])
    lx.got_x()
    lx.got_y()
    line_hop("dA", down_block, x, 1)
    gate_chunk(1)
    down_sum.step(1, 0)
    line_hop("dA", down_block, x, 2)
    line_first("dB", lambda: down_block(z, ox), down_block, ox)
    down_sum.compute(1, lambda: squared[...])
    down_sum.step(2, 0)
    line_hop("dA", down_block, x, 3)
    lx.got_xy()
    lx.whole()
    line_hop("dB", down_block, ox, 1)
    later_copies = [later_chunk(0, staged)]
    down_sum.step(3, 0)
    later_copies.append(later_chunk(1, squared))
    gathers = len(pending)
    down_sum.step(1, 1)
    line_hop("dB", down_block, ox, 2)
    down_sum.step(2, 1)
    down_copy.wait()
    line_hop("dB", down_block, ox, 3)
    slope_chunk(0)
    up_sum.compute(0, lambda: gate[:, cols_of(0)])
    down_sum.step(3, 1)
    slope_chunk(1)
    up_sum.compute(1, lambda: gate[:, cols_of(1)])
    drain(0, gathers)
    for device in (at_x, at_y, at_k):
        pl.semaphore_signal(ready_sem, inc=1, device_id=device, device_id_type=MESH)
    product = Partial("po", hidden, down_w, ((1,), (0,)), later_x, parts_got, last_got, later_out)
    back = Partial(
        "pb",
        gate,
        up_w,
        ((1,), (1,)),
        cot_x,
        earlier_x,
        earlier_x.at[span(0, tokens), span(3 * feats, feats)],
        grad_out,
    )
    up_sum.step(1, 0)
    product.compute(0)
    product.after_k(0)
    product.compute(1)
    product.after_k(1)
    up_sum.step(2, 0)
    pl.semaphore_wait(ready_sem, 3)
    back.compute(0)
    back.after_k(0)
    up_sum.step(3, 0)
    product.after_y(0)
    back.compute(1)
    back.after_k(1)
    up_sum.step(1, 1)
    product.after_y(1)
    product.finish()
    up_sum.step(2, 1)
    back.after_y(0)
    up_sum.step(3, 1)
    back.after_y(1)
    back.finish()
    for j in range(chunks):
        arrived(preact_out.at[:, span(ox * width + j * cw, cw)], sid(f"pre{j}"))
    down_sum.finish()
    up_sum.finish()
    for copy in later_copies + locals_:
        copy.wait()
    drain(gathers, len(pending))


def on_device_rings(
    later_input, earlier_input, cotangent, up_weight, down_weight, up_running, down_running
):
    n = lax.axis_size("fs")
    factor = float(later_input.shape[0] * n) ** (-0.5)

    up_full, up_arrived = ring_gather(up_weight)
    inputs = tp_gather(jnp.stack((later_input, earlier_input, cotangent)))
    later_full, earlier_full, cot_full = inputs[0], inputs[1], inputs[2]
    down_rows = after(down_weight.T, inputs, *up_arrived[-4])
    down_full, down_arrived = ring_gather(down_rows)

    earlier_up = jnp.dot(earlier_full, up_full, preferred_element_type=jnp.float32)
    earlier_relu = jax.nn.relu(earlier_up)
    earlier_hidden = jnp.square(earlier_relu).astype(jnp.bfloat16)
    down_terms = lax.dot_general(
        cot_full, earlier_hidden, contract_first, preferred_element_type=jnp.float32
    ).astype(jnp.bfloat16)
    down_sum = ring_scatter(down_terms, down_arrived[-4])

    later_up = jnp.dot(later_full, up_full, preferred_element_type=jnp.float32)
    later_preact = later_up.astype(jnp.bfloat16)
    later_hidden = jnp.square(jax.nn.relu(later_up)).astype(jnp.bfloat16)

    grad = jnp.dot(cot_full, down_full, preferred_element_type=jnp.float32)
    up_grad = (2.0 * earlier_relu * grad).astype(jnp.bfloat16)
    up_terms = lax.dot_general(
        earlier_full, up_grad, contract_first, preferred_element_type=jnp.float32
    ).astype(jnp.bfloat16)
    up_sum = ring_scatter(up_terms)

    back_part = lax.dot_general(
        up_grad, up_full, contract_last, preferred_element_type=jnp.float32
    ).astype(jnp.bfloat16)
    product = lax.dot_general(
        later_hidden, down_full, contract_last, preferred_element_type=jnp.float32
    ).astype(jnp.bfloat16)
    return (
        tp_scatter(product),
        later_preact,
        tp_scatter(back_part),
        up_running + up_sum * factor,
        down_running + down_sum * factor,
    )


def across_x(n_fs):
    return 1 << ((n_fs.bit_length() - 1) // 2)


def on_device_kernel(
    later_input, earlier_input, cotangent, up_weight, down_weight, up_running, down_running
):
    n = lax.axis_size("fs")
    nz = n // 2
    tokens, feats = later_input.shape
    fan, width = up_weight.shape[0], up_weight.shape[1] // 2
    depth, rows = n * fan, 2 * tokens
    factor = float(tokens * n) ** (-0.5)
    bf16 = jnp.bfloat16
    semaphores = 160
    anywhere = pl.BlockSpec(memory_space=pl.ANY)
    later_output, later_preact, earlier_grad, up_sum, down_sum = pl.pallas_call(
        functools.partial(layer_kernel, nz),
        out_shape=(
            jax.ShapeDtypeStruct((tokens, feats), bf16),
            jax.ShapeDtypeStruct((tokens, 2 * width), bf16),
            jax.ShapeDtypeStruct((tokens, feats), bf16),
            jax.ShapeDtypeStruct((fan, 2 * width), bf16),
            jax.ShapeDtypeStruct((fan, 2 * width), bf16),
        ),
        in_specs=[anywhere] * 5,
        out_specs=(anywhere,) * 5,
        scratch_shapes=[
            pltpu.VMEM((rows, depth), bf16),
            pltpu.VMEM((rows, depth), bf16),
            pltpu.VMEM((rows, depth), bf16),
            pltpu.VMEM((depth, width), bf16),
            pltpu.VMEM((width, depth), bf16),
            pltpu.VMEM((rows, width), bf16),
            pltpu.VMEM((rows, width), bf16),
            pltpu.VMEM((rows, width // 2), bf16),
            pltpu.VMEM((rows, width // 2), bf16),
            pltpu.VMEM((depth, width), bf16),
            pltpu.VMEM((depth, width), bf16),
            pltpu.VMEM((nz + 1, 2 * fan, width), bf16),
            pltpu.VMEM((nz + 1, 2 * fan, width), bf16),
            pltpu.VMEM((rows, 3 * feats), bf16),
            pltpu.VMEM((tokens, feats), bf16),
            pltpu.SemaphoreType.DMA((semaphores,)),
            pltpu.SemaphoreType.DMA((semaphores,)),
            pltpu.SemaphoreType.DMA((semaphores,)),
            pltpu.SemaphoreType.REGULAR,
        ],
        compiler_params=pltpu.CompilerParams(
            collective_id=0, has_side_effects=True, vmem_limit_bytes=VMEM_BYTES
        ),
        name="layer",
    )(later_input, earlier_input, cotangent, up_weight, down_weight)
    return (
        later_output,
        later_preact,
        earlier_grad,
        up_running + up_sum.astype(jnp.float32) * factor,
        down_running + down_sum.astype(jnp.float32) * factor,
    )


def on_device(*arrays):
    square = across_x(lax.axis_size("fs")) == 2 and lax.axis_size("tp") == 4
    return (on_device_kernel if square else on_device_rings)(*arrays)


def solution(mesh):
    in_specs = (
        P("fs", "tp"),
        P("fs", "tp"),
        P("fs", "tp"),
        P("fs", "tp"),
        P("tp", "fs"),
        P("fs", "tp"),
        P("fs", "tp"),
    )
    out_specs = (P("fs", "tp"), P("fs", "tp"), P("fs", "tp"), P("fs", "tp"), P("fs", "tp"))
    return jax.shard_map(
        on_device, mesh=mesh, in_specs=in_specs, out_specs=out_specs, check_vma=False
    )
```

```python
import functools
import math

import jax
import jax.numpy as jnp
from jax import lax
from jax.experimental import pallas as pl
from jax.experimental.pallas import tpu as pltpu
from jax.sharding import PartitionSpec as P

contract_last = (((1,), (1,)), ((), ()))
contract_first = (((0,), (0,)), ((), ()))


STREAMS = 4


def ring_index(place, n):
    place = lax.rem(place + 2 * n, n)
    return jnp.where(place < n // 2, 2 * place, 2 * (n - place) - 1)


def ring_pairs(n, direction):
    order = [q * 2 if q < n // 2 else 2 * (n - q) - 1 for q in range(n)]
    return [(order[q], order[(q + direction) % n]) for q in range(n)]


def my_place(n):
    me = lax.axis_index("fs")
    half = lax.div(me, 2)
    return jnp.where(lax.rem(me, 2) == 0, half, n - 1 - half)


def after(value, *others):
    return lax.optimization_barrier((value, *others))[0]


def ring_gather(shard):
    n = lax.axis_size("fs")
    rows, columns = shard.shape
    place = my_place(n)
    blocks = shard.reshape(STREAMS, rows // STREAMS, columns)
    held = [blocks[s : s + 1] for s in range(STREAMS)]
    full = jnp.zeros((n, STREAMS, rows // STREAMS, columns), shard.dtype)
    full = lax.dynamic_update_slice(full, blocks[None], (lax.axis_index("fs"), 0, 0, 0))
    arrived = []
    for step in range(1, n):
        for s in range(STREAMS):
            direction = 1 if s % 2 == 0 else -1
            held[s] = lax.ppermute(held[s], "fs", ring_pairs(n, direction))
            owner = ring_index(place - direction * step, n)
            full = lax.dynamic_update_slice(full, held[s][None], (owner, s, 0, 0))
        arrived.append(tuple(held))
    return full.reshape(n * rows, columns), arrived


def ring_scatter(terms, wait_for=()):
    n = lax.axis_size("fs")
    rows, columns = terms.shape[0] // n, terms.shape[1]
    place = my_place(n)
    blocks = terms.reshape(n, STREAMS, rows // STREAMS, columns)

    def own(s, direction, step):
        owner = ring_index(place - direction * (step + 1), n)
        return lax.dynamic_slice(
            blocks, (owner, s, 0, 0), (1, 1, rows // STREAMS, columns)
        ).reshape(rows // STREAMS, columns)

    totals = [own(s, 1 if s % 2 == 0 else -1, 0) for s in range(STREAMS)]
    if wait_for:
        totals = [after(total, *wait_for) for total in totals]
    for step in range(1, n):
        for s in range(STREAMS):
            direction = 1 if s % 2 == 0 else -1
            got = lax.ppermute(
                totals[s].astype(jnp.bfloat16), "fs", ring_pairs(n, direction)
            )
            totals[s] = got.astype(jnp.float32) + own(s, direction, step).astype(jnp.float32)
    return jnp.concatenate(totals, axis=0)


def flip_pairs(n, mask):
    return [(i, i ^ mask) for i in range(n)]


def tp_gather(block):
    n = lax.axis_size("tp")
    me = lax.axis_index("tp")
    blocks = [block]
    mask = n // 2
    while mask:
        upper = (me & mask) != 0
        merged = []
        for mine in blocks:
            other = lax.ppermute(mine, "tp", flip_pairs(n, mask))
            merged += [jnp.where(upper, other, mine), jnp.where(upper, mine, other)]
        blocks = merged
        mask //= 2
    return jnp.concatenate(blocks, axis=-1)


def tp_scatter(terms):
    n = lax.axis_size("tp")
    me = lax.axis_index("tp")
    width = terms.shape[1] // n
    blocks = [terms[:, j * width : (j + 1) * width] for j in range(n)]
    mask = 1
    while mask < n:
        upper = (me & mask) != 0
        kept = []
        for low, high in zip(blocks[0::2], blocks[1::2]):
            sent = jnp.where(upper, low, high).astype(jnp.bfloat16)
            mine = jnp.where(upper, high, low)
            got = lax.ppermute(sent, "tp", flip_pairs(n, mask))
            kept.append(mine.astype(jnp.float32) + got.astype(jnp.float32))
        blocks = kept
        mask *= 2
    return blocks[0].astype(jnp.bfloat16)


MESH = pl.DeviceIdType.MESH
VMEM_BYTES = 67043328


def span(start, size):
    if not isinstance(start, int):
        start = pl.multiple_of(start, size)
    return pl.ds(start, size)


def layer_kernel(
    nz,
    later_in,
    earlier_in,
    cot_in,
    up_in,
    down_in,
    later_out,
    preact_out,
    grad_out,
    up_out,
    down_out,
    later_x,
    earlier_x,
    cot_x,
    up_w,
    down_w,
    gate,
    hidden,
    squared,
    staged,
    down_terms,
    up_terms,
    down_got,
    up_got,
    parts_got,
    last_got,
    send_sem,
    recv_sem,
    local_sem,
    ready_sem,
):
    fs, tp = lax.axis_index("fs"), lax.axis_index("tp")
    z, x = lax.div(fs, 2), lax.rem(fs, 2)
    y, k = lax.div(tp, 2), lax.rem(tp, 2)
    ox, oy, ok = 1 - x, 1 - y, 1 - k
    at_x, at_y, at_k = (z * 2 + ox, tp), (fs, oy * 2 + k), (fs, y * 2 + ok)
    at_up, at_down = (fs + 2, tp), (fs - 2, tp)
    top = nz - 1

    tokens, feats = later_in.shape
    fan = up_in.shape[0]
    width = up_w.shape[1]
    slab = 2 * fan
    chunks = 2
    cw = width // chunks
    tile = math.gcd(tokens, slab)

    ids = {}
    pending = []

    def sid(name, count=1):
        if name not in ids:
            ids[name] = sum(c for _, c in ids.values()), count
        return ids[name][0]

    def remote(src, dst, index, device):
        return pltpu.make_async_remote_copy(
            src_ref=src,
            dst_ref=dst,
            send_sem=send_sem.at[index],
            recv_sem=recv_sem.at[index],
            device_id=device,
            device_id_type=MESH,
        )

    def send(src, dst, index, device, when=None):
        def go():
            remote(src(), dst(), index, device).start()

        if when is None:
            go()
        else:
            pl.when(when)(go)
        pending.append((src, dst, index, device, when))

    def sent(entry):
        src, dst, index, device, when = entry

        def go():
            remote(src(), dst(), index, device).wait_send()

        if when is None:
            go()
        else:
            pl.when(when)(go)

    def arrived(dst, index):
        remote(dst, dst, index, at_x).wait_recv()

    barrier = pltpu.get_barrier_semaphore()
    for device in (at_x, at_y, at_k):
        pl.semaphore_signal(barrier, inc=1, device_id=device, device_id_type=MESH)

    @pl.when(z > 0)
    def _():
        pl.semaphore_signal(barrier, inc=1, device_id=at_down, device_id_type=MESH)

    @pl.when(z < top)
    def _():
        pl.semaphore_signal(barrier, inc=1, device_id=at_up, device_id_type=MESH)

    pl.semaphore_wait(barrier, 3 + jnp.where(z > 0, 1, 0) + jnp.where(z < top, 1, 0))

    def block(ref, xx, yy, kk):
        return ref.at[span(xx * tokens, tokens), span((yy * 2 + kk) * feats, feats)]

    def up_block(zz, xx, c):
        return up_w.at[span((zz * 2 + xx) * fan, fan), span(c * cw, cw)]

    def down_block(zz, xx, c):
        return down_w.at[span(c * cw, cw), span((zz * 2 + xx) * fan, fan)]

    class Line:
        def __init__(self, name, c, xx, place, own=None):
            self.base = sid(f"{name}{c}", 2 * nz)
            self.place = lambda zz: place(zz, xx, c)
            self.own = own or (lambda: self.place(z))

        def first(self):
            here = lambda: self.place(z)
            send(self.own, here, self.base, at_up, z < top)
            send(self.own, here, self.base + nz, at_down, z > 0)

        def inner(self, h):
            low, high = z * 2 < nz, z * 2 >= nz

            @pl.when(high & (z >= h))
            def _():
                arrived(self.place(z - h), self.base + h - 1)

            @pl.when(low & (z + h <= top))
            def _():
                arrived(self.place(z + h), self.base + nz + h - 1)

            if h < top:
                here, there = lambda: self.place(z - h), lambda: self.place(z + h)
                send(here, here, self.base + h, at_up, high & (z >= h) & (z < top))
                send(there, there, self.base + nz + h, at_down, low & (z + h <= top) & (z > 0))

        def outer(self, h):
            low, high = z * 2 < nz, z * 2 >= nz
            here, there = lambda: self.place(z - h), lambda: self.place(z + h)

            @pl.when(low & (z >= h))
            def _():
                arrived(self.place(z - h), self.base + h - 1)

            send(here, here, self.base + h, at_up, low & (z >= h))

            @pl.when(high & (z + h <= top))
            def _():
                arrived(self.place(z + h), self.base + nz + h - 1)

            send(there, there, self.base + nz + h, at_down, high & (z + h <= top))

    class Rows:
        def __init__(self, name, own, full, both):
            self.name, self.own, self.full, self.both, self.sends = name, own, full, both, []
            self.copy = pltpu.make_async_copy(own, block(full, x, y, k), local_sem.at[sid("local " + name)])

        def local(self):
            self.copy.start()

        def part(self, xx, yy, kk, half):
            if half is None:
                return block(self.full, xx, yy, kk)
            cols = span((yy * 2 + kk) * feats + half * (feats // 2), feats // 2)
            return self.full.at[span(xx * tokens, tokens), cols]

        def to(self, way, source, xx, yy, device, half=None):
            here = lambda: self.part(xx, yy, k, half)
            send((lambda: self.own) if source else here, here, sid(self.name + way), device)
            self.sends.append(pending.pop())

        def first_x(self):
            self.to("x", True, x, y, at_x)

        def first_y(self):
            self.to("y", True, x, y, at_y)

        def first_k(self):
            self.to("k0", True, x, y, at_k)

        def got_x(self):
            arrived(self.part(ox, y, k, None), sid(self.name + "x"))
            self.to("ya", False, ox, y, at_y, 0 if self.both else None)
            self.to("k1", False, ox, y, at_k)

        def got_y(self):
            arrived(self.part(x, oy, k, None), sid(self.name + "y"))
            if self.both:
                self.to("xb", False, x, oy, at_x, 1)
            self.to("k2", False, x, oy, at_k)

        def got_ya(self):
            half = 0 if self.both else None
            arrived(self.part(ox, oy, k, half), sid(self.name + "ya"))
            self.to("k3a", False, ox, oy, at_k, half)

        def got_xb(self):
            arrived(self.part(ox, oy, k, 1), sid(self.name + "xb"))
            self.to("k3b", False, ox, oy, at_k, 1)

        def whole(self):
            self.copy.wait()
            for way, xx, yy in (("k0", x, y), ("k1", ox, y), ("k2", x, oy)):
                arrived(self.part(xx, yy, ok, None), sid(self.name + way))
            for half, way in ((0, "k3a"), (1, "k3b")) if self.both else ((None, "k3a"),):
                arrived(self.part(ox, oy, ok, half), sid(self.name + way))

    ex = Rows("ex", earlier_in, earlier_x, False)
    ct = Rows("ct", cot_in, cot_x, False)
    lx = Rows("lx", later_in, later_x, False)
    own_cols = lambda xx, c: up_in.at[:, span(xx * width + c * cw, cw)]
    own_rows = lambda xx, c: down_in.at[span(xx * width + c * cw, cw), :]
    up_a = [Line("uA", c, x, up_block, lambda c=c: own_cols(x, c)) for c in range(chunks)]
    up_b = [Line("uB", c, ox, up_block) for c in range(chunks)]
    down_a = [Line("dA", c, x, down_block, lambda c=c: own_rows(x, c)) for c in range(chunks)]
    down_b = [Line("dB", c, ox, down_block) for c in range(chunks)]
    copies = []
    for c in range(chunks):
        for source, dest, name in (
            (own_cols(x, c), up_block(z, x, c), "u"),
            (own_rows(x, c), down_block(z, x, c), "d"),
        ):
            copies.append(
                pltpu.make_async_copy(source, dest, local_sem.at[sid(f"local {name}{c}")])
            )

    def swap_up(c):
        send(lambda: own_cols(ox, c), lambda: up_block(z, x, c), sid(f"ux{c}"), at_x)

    def swap_down(c):
        send(lambda: own_rows(ox, c), lambda: down_block(z, x, c), sid(f"dx{c}"), at_x)

    def swapped_up(c):
        arrived(up_block(z, ox, c), sid(f"ux{c}"))
        up_b[c].first()

    def swapped_down(c):
        arrived(down_block(z, ox, c), sid(f"dx{c}"))
        down_b[c].first()

    def dot(a, b, dims):
        return lax.dot_general(a, b, (dims, ((), ())), preferred_element_type=jnp.float32)

    row_tiles = 2 * tokens // tile

    def gate_chunk(j):
        @pl.loop(0, row_tiles)
        def _(i):
            rows, cols = span(i * tile, tile), span(j * cw, cw)
            value = jnp.maximum(dot(earlier_x[rows, :], up_w[:, cols], ((1,), (0,))), 0.0)
            gate[rows, cols] = value.astype(jnp.bfloat16)
            squared[rows, :] = (value * value).astype(jnp.bfloat16)

    def later_chunk(j, place):
        cols = span(j * cw, cw)

        @pl.loop(0, row_tiles)
        def _(i):
            rows = span(i * tile, tile)
            value = dot(later_x[rows, :], up_w[:, cols], ((1,), (0,)))
            place[rows, :] = value.astype(jnp.bfloat16)
            value = jnp.maximum(value, 0.0)
            hidden[rows, cols] = (value * value).astype(jnp.bfloat16)

        out_cols = span(x * width + j * cw, cw)
        send(
            lambda: place.at[span(ox * tokens, tokens), :],
            lambda: preact_out.at[:, out_cols],
            sid(f"pre{j}"),
            at_x,
        )
        copy = pltpu.make_async_copy(
            place.at[span(x * tokens, tokens), :],
            preact_out.at[:, out_cols],
            local_sem.at[sid(f"local pre{j}")],
        )
        copy.start()
        return copy

    def slope_chunk(j):
        @pl.loop(0, row_tiles)
        def _(i):
            rows, cols = span(i * tile, tile), span(j * cw, cw)
            value = dot(cot_x[rows, :], down_w[cols, :], ((1,), (1,)))
            value = 2.0 * gate[rows, cols].astype(jnp.float32) * value
            gate[rows, cols] = value.astype(jnp.bfloat16)

    class Sum:
        def __init__(self, name, left, terms, got, out):
            self.name, self.left, self.terms, self.got, self.out = name, left, terms, got, out

        def rows(self, o, q):
            return span(o * slab + (ox, x)[q] * fan, fan)

        def part(self, o, j, q):
            return self.terms.at[self.rows(o, q), span(j * cw, cw)]

        def slot(self, s, j, q):
            return self.got.at[s, span(q * fan, fan), span(j * cw, cw)]

        def compute(self, j, right):
            for s in range(nz):
                o = jnp.where(z * 2 < nz, top - s, s)
                for q in range(2):
                    self.piece(o, j, q, right)
                    if s < top:
                        self.push(top - s, j, q, 1, z == 0)
                        self.push(s, j, q, -1, z == top)

        def piece(self, o, j, q, right):
            value = dot(self.left[:, self.rows(o, q)], right(), ((0,), (0,)))
            self.terms[self.rows(o, q), span(j * cw, cw)] = value.astype(jnp.bfloat16)

        def push(self, o, j, q, way, when):
            base = sid(f"{self.name}{j}{q}", 2 * nz)
            index, s, device = (base + o, o + 1, at_up) if way > 0 else (base + nz + o, o, at_down)
            send(lambda: self.part(o, j, q), lambda: self.slot(s, j, q), index, device, when)

        def add(self, o, s, j, q):
            value = self.part(o, j, q)[...].astype(jnp.float32)
            value = value + self.slot(s, j, q)[...].astype(jnp.float32)
            self.terms[self.rows(o, q), span(j * cw, cw)] = value.astype(jnp.bfloat16)

        def step(self, t, j, q):
            base = sid(f"{self.name}{j}{q}", 2 * nz)
            up = top - t + z
            down = z - (top - t)

            @pl.when((z >= 1) & (t >= z))
            def _():
                arrived(self.slot(up + 1, j, q), base + up)
                self.add(up, up + 1, j, q)

            if t < top:
                self.push(up, j, q, 1, (z >= 1) & (t >= z))

            @pl.when((z < top) & (t >= top - z))
            def _():
                arrived(self.slot(down, j, q), base + nz + down)
                self.add(down, down, j, q)

            if t < top:
                self.push(down, j, q, -1, (z < top) & (t >= top - z))
                return
            out_cols = span(x * width + j * cw, cw)
            if q == 0:
                send(
                    lambda: self.part(z, j, 0),
                    lambda: self.out.at[:, out_cols],
                    sid(f"{self.name}x{j}"),
                    at_x,
                )
            else:
                copy = pltpu.make_async_copy(
                    self.part(z, j, 1),
                    self.out.at[:, out_cols],
                    local_sem.at[sid(f"local {self.name}{j}")],
                )
                copy.start()
                locals_.append(copy)

        def finish(self):
            for j in range(chunks):
                arrived(
                    self.out.at[:, span(ox * width + j * cw, cw)], sid(f"{self.name}x{j}")
                )

    class Partial:
        def __init__(self, name, left, right, dims, total, got, last, out, both):
            self.both = both
            self.name, self.left, self.right, self.dims = name, left, right, dims
            self.total, self.got, self.last, self.out = total, got, last, out

        def rows(self, h):
            return ox if h == 0 else x

        def tile_of(self, h, yy, kk):
            return self.total.at[
                span(self.rows(h) * tokens, tokens), span((yy * 2 + kk) * feats, feats)
            ]

        def half_of(self, h, yy, half):
            if half is None:
                return self.tile_of(h, yy, k)
            cols = span((yy * 2 + k) * feats + half * (feats // 2), feats // 2)
            return self.total.at[span(self.rows(h) * tokens, tokens), cols]

        def slot(self, h, c):
            return self.got.at[span(h * tokens, tokens), span(c * feats, feats)]

        def half_slot(self, way):
            if not self.both:
                return self.last if way == "x3" else self.slot(int(way[1]) - 1, 2)
            n = ("y1", "y2", "y3", "x1", "x2", "x3").index(way)
            if n < 4:
                cols = span(2 * feats + (n % 2) * (feats // 2), feats // 2)
                return self.got.at[span((n // 2) * tokens, tokens), cols]
            return self.last.at[:, span((n % 2) * (feats // 2), feats // 2)]

        def columns(self, h, kk):
            for yy in range(2):
                cols = span((yy * 2 + kk) * feats, feats)

                @pl.loop(0, tokens // tile)
                def _(i):
                    rows = span(self.rows(h) * tokens + i * tile, tile)
                    right = self.right[cols, :] if self.dims == ((1,), (1,)) else self.right[:, cols]
                    value = dot(self.left[rows, :], right, self.dims)
                    self.total[rows, cols] = value.astype(jnp.bfloat16)

        def compute(self, h):
            self.columns(h, ok)
            for yy in range(2):
                send(
                    lambda yy=yy: self.tile_of(h, yy, ok),
                    lambda yy=yy: self.slot(h, yy),
                    sid(f"{self.name}k{h}{yy}"),
                    at_k,
                )
            self.columns(h, k)

        def add(self, mine, got):
            @pl.loop(0, tokens // tile)
            def _(i):
                rows = span(i * tile, tile)
                value = mine[rows, :].astype(jnp.float32) + got[rows, :].astype(jnp.float32)
                mine[rows, :] = value.astype(jnp.bfloat16)

        def pass_on(self, way, h, yy, half):
            send(
                lambda: self.half_of(h, yy, half),
                lambda: self.half_slot(way),
                sid(self.name + way),
                at_y if way[0] == "y" else at_x,
            )

        def take(self, way, h, yy, half):
            arrived(self.half_slot(way), sid(self.name + way))
            self.add(self.half_of(h, yy, half), self.half_slot(way))

        def after_k(self, h):
            for yy in range(2):
                arrived(self.slot(h, yy), sid(f"{self.name}k{h}{yy}"))
            self.add(self.tile_of(h, oy, k), self.slot(h, oy))
            half = 0 if self.both else None
            self.pass_on(f"y{h + 1}", h, oy, half)
            if h == 0 and self.both:
                self.pass_on("x1", 0, oy, 1)
            self.add(self.tile_of(h, y, k), self.slot(h, y))
            if h == 0 and self.both:
                self.pass_on("x2", 0, y, 1)

        def second(self):
            half = None
            if self.both:
                half = 0
                self.take("x1", 1, oy, 1)
                self.pass_on("y3", 1, oy, 1)
            self.take("y1", 0, y, half)
            self.pass_on("x3", 0, y, half)

        def finish(self):
            if self.both:
                self.take("x2", 1, y, 1)
                self.take("y3", 1, y, 1)
            half = 0 if self.both else None
            self.take("y2", 1, y, half)
            self.take("x3", 1, y, half)
            copy = pltpu.make_async_copy(
                self.tile_of(1, y, k), self.out, local_sem.at[sid(f"local {self.name}")]
            )
            copy.start()
            locals_.append(copy)

    locals_ = []
    down_sum = Sum("ds", cot_x, down_terms, down_got, down_out)
    up_sum = Sum("us", earlier_x, up_terms, up_got, up_out)
    cols_of = lambda j: span(j * cw, cw)

    product = Partial("po", hidden, down_w, ((1,), (0,)), later_x, parts_got, last_got, later_out, False)
    back = Partial(
        "pb",
        gate,
        up_w,
        ((1,), (1,)),
        cot_x,
        earlier_x,
        earlier_x.at[span(0, tokens), span(3 * feats, feats)],
        grad_out,
        False,
    )
    def settle_later():
        for entry in lx.sends:
            sent(entry)

    def settle_cot():
        for entry in ct.sends:
            sent(entry)

    def settle_earlier():
        for entry in ex.sends:
            sent(entry)
        for device in (at_x, at_y, at_k):
            pl.semaphore_signal(ready_sem, inc=1, device_id=device, device_id_type=MESH)

    def others_ready():
        pl.semaphore_wait(ready_sem, 3)

    later_copies = []
    down_a[0].first()
    ct.first_y()
    swap_up(0)
    up_a[1].first()
    swap_down(0)
    ex.first_x()
    swap_up(1)
    up_a[0].first()
    down_a[1].first()
    for copy in copies:
        copy.start()
    ex.local()
    ct.local()
    lx.local()
    swapped_up(0)
    ct.got_y()
    up_a[0].inner(1)
    lx.first_k()
    up_a[0].outer(1)
    ex.first_y()
    up_b[0].inner(1)
    ex.got_x()
    ct.first_x()
    swap_down(1)
    ex.got_y()
    up_a[1].outer(1)
    up_b[0].outer(1)
    ct.first_k()
    up_a[0].inner(2)
    up_a[1].inner(1)
    lx.first_x()
    up_a[1].inner(2)
    up_b[0].inner(2)
    ct.got_x()
    swapped_up(1)
    ex.got_ya()
    up_a[0].inner(3)
    up_b[1].outer(1)
    swapped_down(0)
    ex.first_k()
    down_a[0].outer(1)
    lx.first_y()
    swapped_down(1)
    down_a[1].outer(1)
    ex.whole()
    up_b[0].inner(3)
    for copy in copies:
        copy.wait()
    gate_chunk(0)
    down_a[0].inner(1)
    ct.got_ya()
    lx.got_x()
    down_b[0].inner(1)
    ct.whole()
    down_sum.compute(0, lambda: squared[...])
    up_b[1].inner(1)
    up_a[1].inner(3)
    up_b[1].inner(2)
    up_b[1].inner(3)
    gate_chunk(1)
    down_b[0].outer(1)
    down_a[0].inner(2)
    down_b[0].inner(2)
    lx.got_y()
    down_sum.compute(1, lambda: squared[...])
    lx.got_ya()
    down_sum.step(1, 0, 1)
    down_a[1].inner(1)
    down_b[1].inner(1)
    lx.whole()
    later_copies.append(later_chunk(1, squared))
    down_sum.step(1, 0, 0)
    down_a[0].inner(3)
    down_b[1].outer(1)
    later_copies.append(later_chunk(0, staged))
    down_a[1].inner(2)
    down_b[0].inner(3)
    slope_chunk(0)
    settle_later()
    down_sum.step(1, 1, 0)
    up_sum.compute(0, lambda: gate[:, cols_of(0)])
    down_b[1].inner(2)
    down_a[1].inner(3)
    down_b[1].inner(3)
    down_sum.step(1, 1, 1)
    product.compute(0)
    down_sum.step(2, 1, 0)
    slope_chunk(1)
    down_sum.step(2, 0, 0)
    product.after_k(0)
    up_sum.compute(1, lambda: gate[:, cols_of(1)])
    settle_cot()
    settle_earlier()
    down_sum.step(2, 0, 1)
    down_sum.step(3, 1, 0)
    down_sum.step(3, 0, 0)
    others_ready()
    back.compute(0)
    back.after_k(0)
    up_sum.step(1, 0, 1)
    product.compute(1)
    product.after_k(1)
    product.second()
    up_sum.step(1, 0, 0)
    up_sum.step(2, 0, 1)
    back.compute(1)
    down_sum.step(2, 1, 1)
    up_sum.step(2, 0, 0)
    up_sum.step(1, 1, 0)
    back.after_k(1)
    back.second()
    down_sum.step(3, 1, 1)
    up_sum.step(1, 1, 1)
    product.finish()
    up_sum.step(2, 1, 0)
    up_sum.step(3, 0, 0)
    up_sum.step(3, 1, 0)
    down_sum.step(3, 0, 1)
    up_sum.step(2, 1, 1)
    up_sum.step(3, 0, 1)
    up_sum.step(3, 1, 1)
    back.finish()
    for j in range(chunks):
        arrived(preact_out.at[:, span(ox * width + j * cw, cw)], sid(f"pre{j}"))
    down_sum.finish()
    up_sum.finish()
    for copy in later_copies + locals_:
        copy.wait()
    for entry in pending:
        sent(entry)


def on_device_rings(
    later_input, earlier_input, cotangent, up_weight, down_weight, up_running, down_running
):
    n = lax.axis_size("fs")
    factor = float(later_input.shape[0] * n) ** (-0.5)

    up_full, up_arrived = ring_gather(up_weight)
    inputs = tp_gather(jnp.stack((later_input, earlier_input, cotangent)))
    later_full, earlier_full, cot_full = inputs[0], inputs[1], inputs[2]
    down_rows = after(down_weight.T, inputs, *up_arrived[-4])
    down_full, down_arrived = ring_gather(down_rows)

    earlier_up = jnp.dot(earlier_full, up_full, preferred_element_type=jnp.float32)
    earlier_relu = jax.nn.relu(earlier_up)
    earlier_hidden = jnp.square(earlier_relu).astype(jnp.bfloat16)
    down_terms = lax.dot_general(
        cot_full, earlier_hidden, contract_first, preferred_element_type=jnp.float32
    ).astype(jnp.bfloat16)
    down_sum = ring_scatter(down_terms, down_arrived[-4])

    later_up = jnp.dot(later_full, up_full, preferred_element_type=jnp.float32)
    later_preact = later_up.astype(jnp.bfloat16)
    later_hidden = jnp.square(jax.nn.relu(later_up)).astype(jnp.bfloat16)

    grad = jnp.dot(cot_full, down_full, preferred_element_type=jnp.float32)
    up_grad = (2.0 * earlier_relu * grad).astype(jnp.bfloat16)
    up_terms = lax.dot_general(
        earlier_full, up_grad, contract_first, preferred_element_type=jnp.float32
    ).astype(jnp.bfloat16)
    up_sum = ring_scatter(up_terms)

    back_part = lax.dot_general(
        up_grad, up_full, contract_last, preferred_element_type=jnp.float32
    ).astype(jnp.bfloat16)
    product = lax.dot_general(
        later_hidden, down_full, contract_last, preferred_element_type=jnp.float32
    ).astype(jnp.bfloat16)
    return (
        tp_scatter(product),
        later_preact,
        tp_scatter(back_part),
        up_running + up_sum * factor,
        down_running + down_sum * factor,
    )


def across_x(n_fs):
    return 1 << ((n_fs.bit_length() - 1) // 2)


def on_device_kernel(
    later_input, earlier_input, cotangent, up_weight, down_weight, up_running, down_running
):
    n = lax.axis_size("fs")
    nz = n // 2
    tokens, feats = later_input.shape
    fan, width = up_weight.shape[0], up_weight.shape[1] // 2
    depth, rows = n * fan, 2 * tokens
    factor = float(tokens * n) ** (-0.5)
    bf16 = jnp.bfloat16
    semaphores = 352
    anywhere = pl.BlockSpec(memory_space=pl.ANY)
    later_output, later_preact, earlier_grad, up_sum, down_sum = pl.pallas_call(
        functools.partial(layer_kernel, nz),
        out_shape=(
            jax.ShapeDtypeStruct((tokens, feats), bf16),
            jax.ShapeDtypeStruct((tokens, 2 * width), bf16),
            jax.ShapeDtypeStruct((tokens, feats), bf16),
            jax.ShapeDtypeStruct((fan, 2 * width), bf16),
            jax.ShapeDtypeStruct((fan, 2 * width), bf16),
        ),
        in_specs=[anywhere] * 5,
        out_specs=(anywhere,) * 5,
        scratch_shapes=[
            pltpu.VMEM((rows, depth), bf16),
            pltpu.VMEM((rows, depth), bf16),
            pltpu.VMEM((rows, depth), bf16),
            pltpu.VMEM((depth, width), bf16),
            pltpu.VMEM((width, depth), bf16),
            pltpu.VMEM((rows, width), bf16),
            pltpu.VMEM((rows, width), bf16),
            pltpu.VMEM((rows, width // 2), bf16),
            pltpu.VMEM((rows, width // 2), bf16),
            pltpu.VMEM((depth, width), bf16),
            pltpu.VMEM((depth, width), bf16),
            pltpu.VMEM((nz + 1, 2 * fan, width), bf16),
            pltpu.VMEM((nz + 1, 2 * fan, width), bf16),
            pltpu.VMEM((rows, 3 * feats), bf16),
            pltpu.VMEM((tokens, feats), bf16),
            pltpu.SemaphoreType.DMA((semaphores,)),
            pltpu.SemaphoreType.DMA((semaphores,)),
            pltpu.SemaphoreType.DMA((semaphores,)),
            pltpu.SemaphoreType.REGULAR,
        ],
        compiler_params=pltpu.CompilerParams(
            collective_id=0, has_side_effects=True, vmem_limit_bytes=VMEM_BYTES
        ),
        name="layer",
    )(later_input, earlier_input, cotangent, up_weight, down_weight)
    return (
        later_output,
        later_preact,
        earlier_grad,
        up_running + up_sum.astype(jnp.float32) * factor,
        down_running + down_sum.astype(jnp.float32) * factor,
    )


def on_device(*arrays):
    square = across_x(lax.axis_size("fs")) == 2 and lax.axis_size("tp") == 4
    return (on_device_kernel if square else on_device_rings)(*arrays)


def solution(mesh):
    in_specs = (
        P("fs", "tp"),
        P("fs", "tp"),
        P("fs", "tp"),
        P("fs", "tp"),
        P("tp", "fs"),
        P("fs", "tp"),
        P("fs", "tp"),
    )
    out_specs = (P("fs", "tp"), P("fs", "tp"), P("fs", "tp"), P("fs", "tp"), P("fs", "tp"))
    return jax.shard_map(
        on_device, mesh=mesh, in_specs=in_specs, out_specs=out_specs, check_vma=False
    )
```

```python
import functools
import math

import jax
import jax.numpy as jnp
from jax import lax
from jax.experimental import pallas as pl
from jax.experimental.pallas import tpu as pltpu
from jax.sharding import PartitionSpec as P

contract_last = (((1,), (1,)), ((), ()))
contract_first = (((0,), (0,)), ((), ()))


STREAMS = 4


def ring_index(place, n):
    place = lax.rem(place + 2 * n, n)
    return jnp.where(place < n // 2, 2 * place, 2 * (n - place) - 1)


def ring_pairs(n, direction):
    order = [q * 2 if q < n // 2 else 2 * (n - q) - 1 for q in range(n)]
    return [(order[q], order[(q + direction) % n]) for q in range(n)]


def my_place(n):
    me = lax.axis_index("fs")
    half = lax.div(me, 2)
    return jnp.where(lax.rem(me, 2) == 0, half, n - 1 - half)


def after(value, *others):
    return lax.optimization_barrier((value, *others))[0]


def ring_gather(shard):
    n = lax.axis_size("fs")
    rows, columns = shard.shape
    place = my_place(n)
    blocks = shard.reshape(STREAMS, rows // STREAMS, columns)
    held = [blocks[s : s + 1] for s in range(STREAMS)]
    full = jnp.zeros((n, STREAMS, rows // STREAMS, columns), shard.dtype)
    full = lax.dynamic_update_slice(full, blocks[None], (lax.axis_index("fs"), 0, 0, 0))
    arrived = []
    for step in range(1, n):
        for s in range(STREAMS):
            direction = 1 if s % 2 == 0 else -1
            held[s] = lax.ppermute(held[s], "fs", ring_pairs(n, direction))
            owner = ring_index(place - direction * step, n)
            full = lax.dynamic_update_slice(full, held[s][None], (owner, s, 0, 0))
        arrived.append(tuple(held))
    return full.reshape(n * rows, columns), arrived


def ring_scatter(terms, wait_for=()):
    n = lax.axis_size("fs")
    rows, columns = terms.shape[0] // n, terms.shape[1]
    place = my_place(n)
    blocks = terms.reshape(n, STREAMS, rows // STREAMS, columns)

    def own(s, direction, step):
        owner = ring_index(place - direction * (step + 1), n)
        return lax.dynamic_slice(
            blocks, (owner, s, 0, 0), (1, 1, rows // STREAMS, columns)
        ).reshape(rows // STREAMS, columns)

    totals = [own(s, 1 if s % 2 == 0 else -1, 0) for s in range(STREAMS)]
    if wait_for:
        totals = [after(total, *wait_for) for total in totals]
    for step in range(1, n):
        for s in range(STREAMS):
            direction = 1 if s % 2 == 0 else -1
            got = lax.ppermute(
                totals[s].astype(jnp.bfloat16), "fs", ring_pairs(n, direction)
            )
            totals[s] = got.astype(jnp.float32) + own(s, direction, step).astype(jnp.float32)
    return jnp.concatenate(totals, axis=0)


def flip_pairs(n, mask):
    return [(i, i ^ mask) for i in range(n)]


def tp_gather(block):
    n = lax.axis_size("tp")
    me = lax.axis_index("tp")
    blocks = [block]
    mask = n // 2
    while mask:
        upper = (me & mask) != 0
        merged = []
        for mine in blocks:
            other = lax.ppermute(mine, "tp", flip_pairs(n, mask))
            merged += [jnp.where(upper, other, mine), jnp.where(upper, mine, other)]
        blocks = merged
        mask //= 2
    return jnp.concatenate(blocks, axis=-1)


def tp_scatter(terms):
    n = lax.axis_size("tp")
    me = lax.axis_index("tp")
    width = terms.shape[1] // n
    blocks = [terms[:, j * width : (j + 1) * width] for j in range(n)]
    mask = 1
    while mask < n:
        upper = (me & mask) != 0
        kept = []
        for low, high in zip(blocks[0::2], blocks[1::2]):
            sent = jnp.where(upper, low, high).astype(jnp.bfloat16)
            mine = jnp.where(upper, high, low)
            got = lax.ppermute(sent, "tp", flip_pairs(n, mask))
            kept.append(mine.astype(jnp.float32) + got.astype(jnp.float32))
        blocks = kept
        mask *= 2
    return blocks[0].astype(jnp.bfloat16)


MESH = pl.DeviceIdType.MESH
VMEM_BYTES = 67043328


def span(start, size):
    if not isinstance(start, int):
        start = pl.multiple_of(start, size)
    return pl.ds(start, size)


def layer_kernel(
    nz,
    later_in,
    earlier_in,
    cot_in,
    up_in,
    down_in,
    later_out,
    preact_out,
    grad_out,
    up_out,
    down_out,
    later_x,
    earlier_x,
    cot_x,
    up_w,
    down_w,
    gate,
    hidden,
    squared,
    staged,
    down_terms,
    up_terms,
    down_got,
    up_got,
    parts_got,
    last_got,
    send_sem,
    recv_sem,
    local_sem,
    ready_sem,
):
    fs, tp = lax.axis_index("fs"), lax.axis_index("tp")
    z, x = lax.div(fs, 2), lax.rem(fs, 2)
    y, k = lax.div(tp, 2), lax.rem(tp, 2)
    ox, oy, ok = 1 - x, 1 - y, 1 - k
    at_x, at_y, at_k = (z * 2 + ox, tp), (fs, oy * 2 + k), (fs, y * 2 + ok)
    at_up, at_down = (fs + 2, tp), (fs - 2, tp)
    top = nz - 1

    tokens, feats = later_in.shape
    fan = up_in.shape[0]
    width = up_w.shape[1]
    slab = 2 * fan
    chunks = 2
    cw = width // chunks
    tile = math.gcd(tokens, slab)

    ids, local_ids = {}, {}
    pending = []

    def sid(name, count=1):
        if name not in ids:
            ids[name] = sum(c for _, c in ids.values()), count
        return ids[name][0]

    def lid(name):
        return local_ids.setdefault(name, len(local_ids))

    def remote(src, dst, index, device):
        return pltpu.make_async_remote_copy(
            src_ref=src,
            dst_ref=dst,
            send_sem=send_sem.at[index],
            recv_sem=recv_sem.at[index],
            device_id=device,
            device_id_type=MESH,
        )

    def send(src, dst, index, device, when=None):
        def go():
            remote(src(), dst(), index, device).start()

        if when is None:
            go()
        else:
            pl.when(when)(go)
        pending.append((src, dst, index, device, when))

    def sent(entry):
        src, dst, index, device, when = entry

        def go():
            remote(src(), dst(), index, device).wait_send()

        if when is None:
            go()
        else:
            pl.when(when)(go)

    def arrived(dst, index):
        remote(dst, dst, index, at_x).wait_recv()

    barrier = pltpu.get_barrier_semaphore()
    for device in (at_x, at_y, at_k):
        pl.semaphore_signal(barrier, inc=1, device_id=device, device_id_type=MESH)

    @pl.when(z > 0)
    def _():
        pl.semaphore_signal(barrier, inc=1, device_id=at_down, device_id_type=MESH)

    @pl.when(z < top)
    def _():
        pl.semaphore_signal(barrier, inc=1, device_id=at_up, device_id_type=MESH)

    pl.semaphore_wait(barrier, 3 + jnp.where(z > 0, 1, 0) + jnp.where(z < top, 1, 0))

    def block(ref, xx, yy, kk):
        return ref.at[span(xx * tokens, tokens), span((yy * 2 + kk) * feats, feats)]

    def up_block(zz, xx, c):
        return up_w.at[span((zz * 2 + xx) * fan, fan), span(c * cw, cw)]

    def down_block(zz, xx, c):
        return down_w.at[span(c * cw, cw), span((zz * 2 + xx) * fan, fan)]

    class Line:
        def __init__(self, name, c, xx, place, own=None):
            self.base = sid(f"{name}{c}", 2 * top)
            self.place = lambda zz: place(zz, xx, c)
            self.own = own or (lambda: self.place(z))

        def first(self):
            here = lambda: self.place(z)
            send(self.own, here, self.base, at_up, z < top)
            send(self.own, here, self.base + top, at_down, z > 0)

        def inner(self, h):
            low, high = z * 2 < nz, z * 2 >= nz

            @pl.when(high & (z >= h))
            def _():
                arrived(self.place(z - h), self.base + h - 1)

            @pl.when(low & (z + h <= top))
            def _():
                arrived(self.place(z + h), self.base + top + h - 1)

            if h < top:
                here, there = lambda: self.place(z - h), lambda: self.place(z + h)
                send(here, here, self.base + h, at_up, high & (z >= h) & (z < top))
                send(there, there, self.base + top + h, at_down, low & (z + h <= top) & (z > 0))

        def outer(self, h):
            low, high = z * 2 < nz, z * 2 >= nz
            here, there = lambda: self.place(z - h), lambda: self.place(z + h)

            @pl.when(low & (z >= h))
            def _():
                arrived(self.place(z - h), self.base + h - 1)

            send(here, here, self.base + h, at_up, low & (z >= h))

            @pl.when(high & (z + h <= top))
            def _():
                arrived(self.place(z + h), self.base + top + h - 1)

            send(there, there, self.base + top + h, at_down, high & (z + h <= top))

    class Rows:
        def __init__(self, name, own, full, both):
            self.name, self.own, self.full, self.both, self.sends = name, own, full, both, []
            self.copy = pltpu.make_async_copy(own, block(full, x, y, k), local_sem.at[lid("local " + name)])

        def local(self):
            self.copy.start()

        def part(self, xx, yy, kk, half):
            if half is None:
                return block(self.full, xx, yy, kk)
            cols = span((yy * 2 + kk) * feats + half * (feats // 2), feats // 2)
            return self.full.at[span(xx * tokens, tokens), cols]

        def to(self, way, source, xx, yy, device, half=None):
            here = lambda: self.part(xx, yy, k, half)
            send((lambda: self.own) if source else here, here, sid(self.name + way), device)
            self.sends.append(pending.pop())

        def first_x(self):
            self.to("x", True, x, y, at_x)

        def first_y(self):
            self.to("y", True, x, y, at_y)

        def first_k(self):
            self.to("k0", True, x, y, at_k)

        def got_x(self):
            arrived(self.part(ox, y, k, None), sid(self.name + "x"))
            self.to("ya", False, ox, y, at_y, 0 if self.both else None)
            self.to("k1", False, ox, y, at_k)

        def got_y(self):
            arrived(self.part(x, oy, k, None), sid(self.name + "y"))
            if self.both:
                self.to("xb", False, x, oy, at_x, 1)
            self.to("k2", False, x, oy, at_k)

        def got_ya(self):
            half = 0 if self.both else None
            arrived(self.part(ox, oy, k, half), sid(self.name + "ya"))
            self.to("k3a", False, ox, oy, at_k, half)

        def got_xb(self):
            arrived(self.part(ox, oy, k, 1), sid(self.name + "xb"))
            self.to("k3b", False, ox, oy, at_k, 1)

        def whole(self):
            self.copy.wait()
            for way, xx, yy in (("k0", x, y), ("k1", ox, y), ("k2", x, oy)):
                arrived(self.part(xx, yy, ok, None), sid(self.name + way))
            for half, way in ((0, "k3a"), (1, "k3b")) if self.both else ((None, "k3a"),):
                arrived(self.part(ox, oy, ok, half), sid(self.name + way))

    ex = Rows("ex", earlier_in, earlier_x, False)
    ct = Rows("ct", cot_in, cot_x, False)
    lx = Rows("lx", later_in, later_x, False)
    own_cols = lambda xx, c: up_in.at[:, span(xx * width + c * cw, cw)]
    own_rows = lambda xx, c: down_in.at[span(xx * width + c * cw, cw), :]
    up_a = [Line("uA", c, x, up_block, lambda c=c: own_cols(x, c)) for c in range(chunks)]
    up_b = [Line("uB", c, ox, up_block) for c in range(chunks)]
    down_a = [Line("dA", c, x, down_block, lambda c=c: own_rows(x, c)) for c in range(chunks)]
    down_b = [Line("dB", c, ox, down_block) for c in range(chunks)]
    copies = []
    for c in range(chunks):
        for source, dest, name in (
            (own_cols(x, c), up_block(z, x, c), "u"),
            (own_rows(x, c), down_block(z, x, c), "d"),
        ):
            copies.append(
                pltpu.make_async_copy(source, dest, local_sem.at[lid(f"local {name}{c}")])
            )

    def swap_up(c):
        send(lambda: own_cols(ox, c), lambda: up_block(z, x, c), sid(f"ux{c}"), at_x)

    def swap_down(c):
        send(lambda: own_rows(ox, c), lambda: down_block(z, x, c), sid(f"dx{c}"), at_x)

    def swapped_up(c):
        arrived(up_block(z, ox, c), sid(f"ux{c}"))
        up_b[c].first()

    def swapped_down(c):
        arrived(down_block(z, ox, c), sid(f"dx{c}"))
        down_b[c].first()

    def dot(a, b, dims):
        return lax.dot_general(a, b, (dims, ((), ())), preferred_element_type=jnp.float32)

    row_tiles = 2 * tokens // tile

    def gate_chunk(j):
        @pl.loop(0, row_tiles)
        def _(i):
            rows, cols = span(i * tile, tile), span(j * cw, cw)
            value = jnp.maximum(dot(earlier_x[rows, :], up_w[:, cols], ((1,), (0,))), 0.0)
            gate[rows, cols] = value.astype(jnp.bfloat16)
            squared[rows, :] = (value * value).astype(jnp.bfloat16)

    def later_chunk(j, place):
        cols = span(j * cw, cw)

        @pl.loop(0, row_tiles)
        def _(i):
            rows = span(i * tile, tile)
            value = dot(later_x[rows, :], up_w[:, cols], ((1,), (0,)))
            place[rows, :] = value.astype(jnp.bfloat16)
            value = jnp.maximum(value, 0.0)
            hidden[rows, cols] = (value * value).astype(jnp.bfloat16)

        out_cols = span(x * width + j * cw, cw)
        send(
            lambda: place.at[span(ox * tokens, tokens), :],
            lambda: preact_out.at[:, out_cols],
            sid(f"pre{j}"),
            at_x,
        )
        copy = pltpu.make_async_copy(
            place.at[span(x * tokens, tokens), :],
            preact_out.at[:, out_cols],
            local_sem.at[lid(f"local pre{j}")],
        )
        copy.start()
        return copy

    def slope_chunk(j):
        @pl.loop(0, row_tiles)
        def _(i):
            rows, cols = span(i * tile, tile), span(j * cw, cw)
            value = dot(cot_x[rows, :], down_w[cols, :], ((1,), (1,)))
            value = 2.0 * gate[rows, cols].astype(jnp.float32) * value
            gate[rows, cols] = value.astype(jnp.bfloat16)

    class Sum:
        def __init__(self, name, left, terms, got, out):
            self.name, self.left, self.terms, self.got, self.out = name, left, terms, got, out

        def rows(self, o, q):
            return span(o * slab + (ox, x)[q] * fan, fan)

        def part(self, o, j, q):
            return self.terms.at[self.rows(o, q), span(j * cw, cw)]

        def slot(self, s, j, q):
            return self.got.at[s, span(q * fan, fan), span(j * cw, cw)]

        def compute(self, j, right):
            for s in range(nz):
                o = jnp.where(z * 2 < nz, top - s, s)
                for q in range(2):
                    self.piece(o, j, q, right)
                    if s < top:
                        self.push(top - s, j, q, 1, z == 0)
                        self.push(s, j, q, -1, z == top)

        def piece(self, o, j, q, right):
            value = dot(self.left[:, self.rows(o, q)], right(), ((0,), (0,)))
            self.terms[self.rows(o, q), span(j * cw, cw)] = value.astype(jnp.bfloat16)

        def push(self, o, j, q, way, when):
            base = sid(f"{self.name}{j}{q}", 2 * top)
            index, s, device = (base + o - 1, o + 1, at_up) if way > 0 else (base + top + o, o, at_down)
            send(lambda: self.part(o, j, q), lambda: self.slot(s, j, q), index, device, when)

        def add(self, o, s, j, q):
            value = self.part(o, j, q)[...].astype(jnp.float32)
            value = value + self.slot(s, j, q)[...].astype(jnp.float32)
            self.terms[self.rows(o, q), span(j * cw, cw)] = value.astype(jnp.bfloat16)

        def step(self, t, j, q):
            base = sid(f"{self.name}{j}{q}", 2 * top)
            up = top - t + z
            down = z - (top - t)

            @pl.when((z >= 1) & (t >= z))
            def _():
                arrived(self.slot(up + 1, j, q), base + up - 1)
                self.add(up, up + 1, j, q)

            if t < top:
                self.push(up, j, q, 1, (z >= 1) & (t >= z))

            @pl.when((z < top) & (t >= top - z))
            def _():
                arrived(self.slot(down, j, q), base + top + down)
                self.add(down, down, j, q)

            if t < top:
                self.push(down, j, q, -1, (z < top) & (t >= top - z))
                return
            out_cols = span(x * width + j * cw, cw)
            if q == 0:
                send(
                    lambda: self.part(z, j, 0),
                    lambda: self.out.at[:, out_cols],
                    sid(f"{self.name}x{j}"),
                    at_x,
                )
            else:
                copy = pltpu.make_async_copy(
                    self.part(z, j, 1),
                    self.out.at[:, out_cols],
                    local_sem.at[lid(f"local {self.name}{j}")],
                )
                copy.start()
                locals_.append(copy)

        def finish(self):
            for j in range(chunks):
                arrived(
                    self.out.at[:, span(ox * width + j * cw, cw)], sid(f"{self.name}x{j}")
                )

    class Partial:
        def __init__(self, name, left, right, dims, total, got, last, out, both):
            self.both = both
            self.name, self.left, self.right, self.dims = name, left, right, dims
            self.total, self.got, self.last, self.out = total, got, last, out

        def rows(self, h):
            return ox if h == 0 else x

        def tile_of(self, h, yy, kk):
            return self.total.at[
                span(self.rows(h) * tokens, tokens), span((yy * 2 + kk) * feats, feats)
            ]

        def half_of(self, h, yy, half):
            if half is None:
                return self.tile_of(h, yy, k)
            cols = span((yy * 2 + k) * feats + half * (feats // 2), feats // 2)
            return self.total.at[span(self.rows(h) * tokens, tokens), cols]

        def slot(self, h, c):
            return self.got.at[span(h * tokens, tokens), span(c * feats, feats)]

        def half_slot(self, way):
            if not self.both:
                return self.last if way == "x3" else self.slot(int(way[1]) - 1, 2)
            n = ("y1", "y2", "y3", "x1", "x2", "x3").index(way)
            if n < 4:
                cols = span(2 * feats + (n % 2) * (feats // 2), feats // 2)
                return self.got.at[span((n // 2) * tokens, tokens), cols]
            return self.last.at[:, span((n % 2) * (feats // 2), feats // 2)]

        def columns(self, h, kk):
            for yy in range(2):
                cols = span((yy * 2 + kk) * feats, feats)

                @pl.loop(0, tokens // tile)
                def _(i):
                    rows = span(self.rows(h) * tokens + i * tile, tile)
                    right = self.right[cols, :] if self.dims == ((1,), (1,)) else self.right[:, cols]
                    value = dot(self.left[rows, :], right, self.dims)
                    self.total[rows, cols] = value.astype(jnp.bfloat16)

        def compute(self, h):
            self.columns(h, ok)
            for yy in range(2):
                send(
                    lambda yy=yy: self.tile_of(h, yy, ok),
                    lambda yy=yy: self.slot(h, yy),
                    sid(f"{self.name}k{h}{yy}"),
                    at_k,
                )
            self.columns(h, k)

        def add(self, mine, got):
            @pl.loop(0, tokens // tile)
            def _(i):
                rows = span(i * tile, tile)
                value = mine[rows, :].astype(jnp.float32) + got[rows, :].astype(jnp.float32)
                mine[rows, :] = value.astype(jnp.bfloat16)

        def pass_on(self, way, h, yy, half):
            send(
                lambda: self.half_of(h, yy, half),
                lambda: self.half_slot(way),
                sid(self.name + way),
                at_y if way[0] == "y" else at_x,
            )

        def take(self, way, h, yy, half):
            arrived(self.half_slot(way), sid(self.name + way))
            self.add(self.half_of(h, yy, half), self.half_slot(way))

        def after_k(self, h):
            for yy in range(2):
                arrived(self.slot(h, yy), sid(f"{self.name}k{h}{yy}"))
            self.add(self.tile_of(h, oy, k), self.slot(h, oy))
            half = 0 if self.both else None
            self.pass_on(f"y{h + 1}", h, oy, half)
            if h == 0 and self.both:
                self.pass_on("x1", 0, oy, 1)
            self.add(self.tile_of(h, y, k), self.slot(h, y))
            if h == 0 and self.both:
                self.pass_on("x2", 0, y, 1)

        def second(self):
            half = None
            if self.both:
                half = 0
                self.take("x1", 1, oy, 1)
                self.pass_on("y3", 1, oy, 1)
            self.take("y1", 0, y, half)
            self.pass_on("x3", 0, y, half)

        def finish(self):
            if self.both:
                self.take("x2", 1, y, 1)
                self.take("y3", 1, y, 1)
            half = 0 if self.both else None
            self.take("y2", 1, y, half)
            self.take("x3", 1, y, half)
            copy = pltpu.make_async_copy(
                self.tile_of(1, y, k), self.out, local_sem.at[lid(f"local {self.name}")]
            )
            copy.start()
            locals_.append(copy)

    locals_ = []
    down_sum = Sum("ds", cot_x, down_terms, down_got, down_out)
    up_sum = Sum("us", earlier_x, up_terms, up_got, up_out)
    cols_of = lambda j: span(j * cw, cw)

    product = Partial("po", hidden, down_w, ((1,), (0,)), later_x, parts_got, last_got, later_out, False)
    back = Partial(
        "pb",
        gate,
        up_w,
        ((1,), (1,)),
        cot_x,
        earlier_x,
        earlier_x.at[span(0, tokens), span(3 * feats, feats)],
        grad_out,
        False,
    )
    def settle_later():
        for entry in lx.sends:
            sent(entry)

    def settle_cot():
        for entry in ct.sends:
            sent(entry)

    def settle_earlier():
        for entry in ex.sends:
            sent(entry)
        for device in (at_x, at_y, at_k):
            pl.semaphore_signal(ready_sem, inc=1, device_id=device, device_id_type=MESH)

    def others_ready():
        pl.semaphore_wait(ready_sem, 3)

    later_copies = []
    down_a[0].first()
    ct.first_y()
    swap_up(0)
    up_a[1].first()
    swap_down(0)
    ex.first_x()
    swap_up(1)
    up_a[0].first()
    down_a[1].first()
    for copy in copies:
        copy.start()
    ex.local()
    ct.local()
    lx.local()
    swapped_up(0)
    ct.got_y()
    up_a[0].inner(1)
    lx.first_k()
    up_a[0].outer(1)
    ex.first_y()
    up_b[0].inner(1)
    ex.got_x()
    ct.first_x()
    swap_down(1)
    ex.got_y()
    up_a[1].outer(1)
    up_b[0].outer(1)
    ct.first_k()
    up_a[0].inner(2)
    up_a[1].inner(1)
    lx.first_x()
    up_a[1].inner(2)
    up_b[0].inner(2)
    ct.got_x()
    swapped_up(1)
    ex.got_ya()
    up_a[0].inner(3)
    up_b[1].outer(1)
    swapped_down(0)
    ex.first_k()
    down_a[0].outer(1)
    lx.first_y()
    swapped_down(1)
    down_a[1].outer(1)
    ex.whole()
    up_b[0].inner(3)
    for copy in copies:
        copy.wait()
    gate_chunk(0)
    down_a[0].inner(1)
    ct.got_ya()
    lx.got_x()
    down_b[0].inner(1)
    ct.whole()
    down_sum.compute(0, lambda: squared[...])
    up_b[1].inner(1)
    up_a[1].inner(3)
    up_b[1].inner(2)
    up_b[1].inner(3)
    gate_chunk(1)
    down_b[0].outer(1)
    down_a[0].inner(2)
    down_b[0].inner(2)
    lx.got_y()
    down_sum.compute(1, lambda: squared[...])
    lx.got_ya()
    down_sum.step(1, 0, 1)
    down_a[1].inner(1)
    down_b[1].inner(1)
    lx.whole()
    later_copies.append(later_chunk(1, squared))
    down_sum.step(1, 0, 0)
    down_a[0].inner(3)
    down_b[1].outer(1)
    later_copies.append(later_chunk(0, staged))
    down_a[1].inner(2)
    down_b[0].inner(3)
    slope_chunk(0)
    settle_later()
    down_sum.step(1, 1, 0)
    up_sum.compute(0, lambda: gate[:, cols_of(0)])
    down_b[1].inner(2)
    down_a[1].inner(3)
    down_b[1].inner(3)
    down_sum.step(1, 1, 1)
    product.compute(0)
    down_sum.step(2, 1, 0)
    slope_chunk(1)
    down_sum.step(2, 0, 0)
    product.after_k(0)
    up_sum.compute(1, lambda: gate[:, cols_of(1)])
    settle_cot()
    settle_earlier()
    down_sum.step(2, 0, 1)
    down_sum.step(3, 1, 0)
    down_sum.step(3, 0, 0)
    others_ready()
    back.compute(0)
    back.after_k(0)
    up_sum.step(1, 0, 1)
    product.compute(1)
    product.after_k(1)
    product.second()
    up_sum.step(1, 0, 0)
    up_sum.step(2, 0, 1)
    back.compute(1)
    down_sum.step(2, 1, 1)
    up_sum.step(2, 0, 0)
    up_sum.step(1, 1, 0)
    back.after_k(1)
    back.second()
    down_sum.step(3, 1, 1)
    up_sum.step(1, 1, 1)
    product.finish()
    up_sum.step(2, 1, 0)
    up_sum.step(3, 0, 0)
    up_sum.step(3, 1, 0)
    down_sum.step(3, 0, 1)
    up_sum.step(2, 1, 1)
    up_sum.step(3, 0, 1)
    up_sum.step(3, 1, 1)
    back.finish()
    for j in range(chunks):
        arrived(preact_out.at[:, span(ox * width + j * cw, cw)], sid(f"pre{j}"))
    down_sum.finish()
    up_sum.finish()
    for copy in later_copies + locals_:
        copy.wait()
    for entry in pending:
        sent(entry)


def on_device_rings(
    later_input, earlier_input, cotangent, up_weight, down_weight, up_running, down_running
):
    n = lax.axis_size("fs")
    factor = float(later_input.shape[0] * n) ** (-0.5)

    up_full, up_arrived = ring_gather(up_weight)
    inputs = tp_gather(jnp.stack((later_input, earlier_input, cotangent)))
    later_full, earlier_full, cot_full = inputs[0], inputs[1], inputs[2]
    down_rows = after(down_weight.T, inputs, *up_arrived[-4])
    down_full, down_arrived = ring_gather(down_rows)

    earlier_up = jnp.dot(earlier_full, up_full, preferred_element_type=jnp.float32)
    earlier_relu = jax.nn.relu(earlier_up)
    earlier_hidden = jnp.square(earlier_relu).astype(jnp.bfloat16)
    down_terms = lax.dot_general(
        cot_full, earlier_hidden, contract_first, preferred_element_type=jnp.float32
    ).astype(jnp.bfloat16)
    down_sum = ring_scatter(down_terms, down_arrived[-4])

    later_up = jnp.dot(later_full, up_full, preferred_element_type=jnp.float32)
    later_preact = later_up.astype(jnp.bfloat16)
    later_hidden = jnp.square(jax.nn.relu(later_up)).astype(jnp.bfloat16)

    grad = jnp.dot(cot_full, down_full, preferred_element_type=jnp.float32)
    up_grad = (2.0 * earlier_relu * grad).astype(jnp.bfloat16)
    up_terms = lax.dot_general(
        earlier_full, up_grad, contract_first, preferred_element_type=jnp.float32
    ).astype(jnp.bfloat16)
    up_sum = ring_scatter(up_terms)

    back_part = lax.dot_general(
        up_grad, up_full, contract_last, preferred_element_type=jnp.float32
    ).astype(jnp.bfloat16)
    product = lax.dot_general(
        later_hidden, down_full, contract_last, preferred_element_type=jnp.float32
    ).astype(jnp.bfloat16)
    return (
        tp_scatter(product),
        later_preact,
        tp_scatter(back_part),
        up_running + up_sum * factor,
        down_running + down_sum * factor,
    )


def across_x(n_fs):
    return 1 << ((n_fs.bit_length() - 1) // 2)


def on_device_kernel(
    later_input, earlier_input, cotangent, up_weight, down_weight, up_running, down_running
):
    n = lax.axis_size("fs")
    nz = n // 2
    tokens, feats = later_input.shape
    fan, width = up_weight.shape[0], up_weight.shape[1] // 2
    depth, rows = n * fan, 2 * tokens
    factor = float(tokens * n) ** (-0.5)
    bf16 = jnp.bfloat16
    semaphores = 32 * (nz - 1) + 45
    anywhere = pl.BlockSpec(memory_space=pl.ANY)
    later_output, later_preact, earlier_grad, up_sum, down_sum = pl.pallas_call(
        functools.partial(layer_kernel, nz),
        out_shape=(
            jax.ShapeDtypeStruct((tokens, feats), bf16),
            jax.ShapeDtypeStruct((tokens, 2 * width), bf16),
            jax.ShapeDtypeStruct((tokens, feats), bf16),
            jax.ShapeDtypeStruct((fan, 2 * width), bf16),
            jax.ShapeDtypeStruct((fan, 2 * width), bf16),
        ),
        in_specs=[anywhere] * 5,
        out_specs=(anywhere,) * 5,
        scratch_shapes=[
            pltpu.VMEM((rows, depth), bf16),
            pltpu.VMEM((rows, depth), bf16),
            pltpu.VMEM((rows, depth), bf16),
            pltpu.VMEM((depth, width), bf16),
            pltpu.VMEM((width, depth), bf16),
            pltpu.VMEM((rows, width), bf16),
            pltpu.VMEM((rows, width), bf16),
            pltpu.VMEM((rows, width // 2), bf16),
            pltpu.VMEM((rows, width // 2), bf16),
            pltpu.VMEM((depth, width), bf16),
            pltpu.VMEM((depth, width), bf16),
            pltpu.VMEM((nz + 1, 2 * fan, width), bf16),
            pltpu.VMEM((nz + 1, 2 * fan, width), bf16),
            pltpu.VMEM((rows, 3 * feats), bf16),
            pltpu.VMEM((tokens, feats), bf16),
            pltpu.SemaphoreType.DMA((semaphores,)),
            pltpu.SemaphoreType.DMA((semaphores,)),
            pltpu.SemaphoreType.DMA((15,)),
            pltpu.SemaphoreType.REGULAR,
        ],
        compiler_params=pltpu.CompilerParams(
            collective_id=0, has_side_effects=True, vmem_limit_bytes=VMEM_BYTES
        ),
        name="layer",
    )(later_input, earlier_input, cotangent, up_weight, down_weight)
    return (
        later_output,
        later_preact,
        earlier_grad,
        up_running + up_sum.astype(jnp.float32) * factor,
        down_running + down_sum.astype(jnp.float32) * factor,
    )


def on_device(*arrays):
    square = across_x(lax.axis_size("fs")) == 2 and lax.axis_size("tp") == 4
    return (on_device_kernel if square else on_device_rings)(*arrays)


def solution(mesh):
    in_specs = (
        P("fs", "tp"),
        P("fs", "tp"),
        P("fs", "tp"),
        P("fs", "tp"),
        P("tp", "fs"),
        P("fs", "tp"),
        P("fs", "tp"),
    )
    out_specs = (P("fs", "tp"), P("fs", "tp"), P("fs", "tp"), P("fs", "tp"), P("fs", "tp"))
    return jax.shard_map(
        on_device, mesh=mesh, in_specs=in_specs, out_specs=out_specs, check_vma=False
    )
```

```python
import functools
import math

import jax
import jax.numpy as jnp
from jax import lax
from jax.experimental import pallas as pl
from jax.experimental.pallas import tpu as pltpu
from jax.sharding import PartitionSpec as P

contract_last = (((1,), (1,)), ((), ()))
contract_first = (((0,), (0,)), ((), ()))


STREAMS = 4


def ring_index(place, n):
    place = lax.rem(place + 2 * n, n)
    return jnp.where(place < n // 2, 2 * place, 2 * (n - place) - 1)


def ring_pairs(n, direction):
    order = [q * 2 if q < n // 2 else 2 * (n - q) - 1 for q in range(n)]
    return [(order[q], order[(q + direction) % n]) for q in range(n)]


def my_place(n):
    me = lax.axis_index("fs")
    half = lax.div(me, 2)
    return jnp.where(lax.rem(me, 2) == 0, half, n - 1 - half)


def after(value, *others):
    return lax.optimization_barrier((value, *others))[0]


def ring_gather(shard):
    n = lax.axis_size("fs")
    rows, columns = shard.shape
    place = my_place(n)
    blocks = shard.reshape(STREAMS, rows // STREAMS, columns)
    held = [blocks[s : s + 1] for s in range(STREAMS)]
    full = jnp.zeros((n, STREAMS, rows // STREAMS, columns), shard.dtype)
    full = lax.dynamic_update_slice(full, blocks[None], (lax.axis_index("fs"), 0, 0, 0))
    arrived = []
    for step in range(1, n):
        for s in range(STREAMS):
            direction = 1 if s % 2 == 0 else -1
            held[s] = lax.ppermute(held[s], "fs", ring_pairs(n, direction))
            owner = ring_index(place - direction * step, n)
            full = lax.dynamic_update_slice(full, held[s][None], (owner, s, 0, 0))
        arrived.append(tuple(held))
    return full.reshape(n * rows, columns), arrived


def ring_scatter(terms, wait_for=()):
    n = lax.axis_size("fs")
    rows, columns = terms.shape[0] // n, terms.shape[1]
    place = my_place(n)
    blocks = terms.reshape(n, STREAMS, rows // STREAMS, columns)

    def own(s, direction, step):
        owner = ring_index(place - direction * (step + 1), n)
        return lax.dynamic_slice(
            blocks, (owner, s, 0, 0), (1, 1, rows // STREAMS, columns)
        ).reshape(rows // STREAMS, columns)

    totals = [own(s, 1 if s % 2 == 0 else -1, 0) for s in range(STREAMS)]
    if wait_for:
        totals = [after(total, *wait_for) for total in totals]
    for step in range(1, n):
        for s in range(STREAMS):
            direction = 1 if s % 2 == 0 else -1
            got = lax.ppermute(
                totals[s].astype(jnp.bfloat16), "fs", ring_pairs(n, direction)
            )
            totals[s] = got.astype(jnp.float32) + own(s, direction, step).astype(jnp.float32)
    return jnp.concatenate(totals, axis=0)


def flip_pairs(n, mask):
    return [(i, i ^ mask) for i in range(n)]


def tp_gather(block):
    n = lax.axis_size("tp")
    me = lax.axis_index("tp")
    blocks = [block]
    mask = n // 2
    while mask:
        upper = (me & mask) != 0
        merged = []
        for mine in blocks:
            other = lax.ppermute(mine, "tp", flip_pairs(n, mask))
            merged += [jnp.where(upper, other, mine), jnp.where(upper, mine, other)]
        blocks = merged
        mask //= 2
    return jnp.concatenate(blocks, axis=-1)


def tp_scatter(terms):
    n = lax.axis_size("tp")
    me = lax.axis_index("tp")
    width = terms.shape[1] // n
    blocks = [terms[:, j * width : (j + 1) * width] for j in range(n)]
    mask = 1
    while mask < n:
        upper = (me & mask) != 0
        kept = []
        for low, high in zip(blocks[0::2], blocks[1::2]):
            sent = jnp.where(upper, low, high).astype(jnp.bfloat16)
            mine = jnp.where(upper, high, low)
            got = lax.ppermute(sent, "tp", flip_pairs(n, mask))
            kept.append(mine.astype(jnp.float32) + got.astype(jnp.float32))
        blocks = kept
        mask *= 2
    return blocks[0].astype(jnp.bfloat16)


MESH = pl.DeviceIdType.MESH
VMEM_BYTES = 67043328
MIB = 1 << 20


def span(start, size):
    if not isinstance(start, int):
        start = pl.multiple_of(start, size)
    return pl.ds(start, size)


def layer_kernel(
    nz,
    factor,
    later_in,
    earlier_in,
    cot_in,
    up_in,
    down_in,
    up_run,
    down_run,
    later_out,
    preact_out,
    grad_out,
    up_out,
    down_out,
    later_x,
    earlier_x,
    cot_x,
    up_w,
    down_w,
    gate,
    hidden,
    squared,
    staged,
    down_terms,
    up_terms,
    down_got,
    up_got,
    parts_got,
    last_got,
    swap_got,
    running,
    send_sem,
    recv_sem,
    local_sem,
    ready_sem,
):
    fs, tp = lax.axis_index("fs"), lax.axis_index("tp")
    z, x = lax.div(fs, 2), lax.rem(fs, 2)
    y, k = lax.div(tp, 2), lax.rem(tp, 2)
    ox, oy, ok = 1 - x, 1 - y, 1 - k
    at_x, at_y, at_k = (z * 2 + ox, tp), (fs, oy * 2 + k), (fs, y * 2 + ok)
    at_up, at_down = (fs + 2, tp), (fs - 2, tp)
    top = nz - 1

    tokens, feats = later_in.shape
    fan = up_in.shape[0]
    width = up_w.shape[1]
    slab = 2 * fan
    chunks = 2
    cw = width // chunks
    tile = math.gcd(tokens, slab)

    ids, local_ids = {}, {}
    pending = []

    def sid(name, count=1):
        if name not in ids:
            ids[name] = sum(c for _, c in ids.values()), count
        return ids[name][0]

    def lid(name):
        return local_ids.setdefault(name, len(local_ids))

    def remote(src, dst, index, device):
        return pltpu.make_async_remote_copy(
            src_ref=src,
            dst_ref=dst,
            send_sem=send_sem.at[index],
            recv_sem=recv_sem.at[index],
            device_id=device,
            device_id_type=MESH,
        )

    def send(src, dst, index, device, when=None):
        def go():
            remote(src(), dst(), index, device).start()

        if when is None:
            go()
        else:
            pl.when(when)(go)
        pending.append((src, dst, index, device, when))

    def sent(entry):
        src, dst, index, device, when = entry

        def go():
            remote(src(), dst(), index, device).wait_send()

        if when is None:
            go()
        else:
            pl.when(when)(go)

    def arrived(dst, index):
        remote(dst, dst, index, at_x).wait_recv()

    barrier = pltpu.get_barrier_semaphore()
    for device in (at_x, at_y, at_k):
        pl.semaphore_signal(barrier, inc=1, device_id=device, device_id_type=MESH)

    @pl.when(z > 0)
    def _():
        pl.semaphore_signal(barrier, inc=1, device_id=at_down, device_id_type=MESH)

    @pl.when(z < top)
    def _():
        pl.semaphore_signal(barrier, inc=1, device_id=at_up, device_id_type=MESH)

    pl.semaphore_wait(barrier, 3 + jnp.where(z > 0, 1, 0) + jnp.where(z < top, 1, 0))

    def block(ref, xx, yy, kk):
        return ref.at[span(xx * tokens, tokens), span((yy * 2 + kk) * feats, feats)]

    def up_block(zz, xx, c):
        return up_w.at[span((zz * 2 + xx) * fan, fan), span(c * cw, cw)]

    def down_block(zz, xx, c):
        return down_w.at[span(c * cw, cw), span((zz * 2 + xx) * fan, fan)]

    class Line:
        def __init__(self, name, c, xx, place, own=None):
            self.base = sid(f"{name}{c}", 2 * top)
            self.place = lambda zz: place(zz, xx, c)
            self.own = own or (lambda: self.place(z))

        def first(self):
            here = lambda: self.place(z)
            send(self.own, here, self.base, at_up, z < top)
            send(self.own, here, self.base + top, at_down, z > 0)

        def inner(self, h):
            low, high = z * 2 < nz, z * 2 >= nz

            @pl.when(high & (z >= h))
            def _():
                arrived(self.place(z - h), self.base + h - 1)

            @pl.when(low & (z + h <= top))
            def _():
                arrived(self.place(z + h), self.base + top + h - 1)

            if h < top:
                here, there = lambda: self.place(z - h), lambda: self.place(z + h)
                send(here, here, self.base + h, at_up, high & (z >= h) & (z < top))
                send(there, there, self.base + top + h, at_down, low & (z + h <= top) & (z > 0))

        def outer(self, h):
            low, high = z * 2 < nz, z * 2 >= nz
            here, there = lambda: self.place(z - h), lambda: self.place(z + h)

            @pl.when(low & (z >= h))
            def _():
                arrived(self.place(z - h), self.base + h - 1)

            send(here, here, self.base + h, at_up, low & (z >= h))

            @pl.when(high & (z + h <= top))
            def _():
                arrived(self.place(z + h), self.base + top + h - 1)

            send(there, there, self.base + top + h, at_down, high & (z + h <= top))

    class Rows:
        def __init__(self, name, own, full, both):
            self.name, self.own, self.full, self.both, self.sends = name, own, full, both, []
            self.copy = pltpu.make_async_copy(own, block(full, x, y, k), local_sem.at[lid("local " + name)])

        def local(self):
            self.copy.start()

        def part(self, xx, yy, kk, half):
            if half is None:
                return block(self.full, xx, yy, kk)
            cols = span((yy * 2 + kk) * feats + half * (feats // 2), feats // 2)
            return self.full.at[span(xx * tokens, tokens), cols]

        def to(self, way, source, xx, yy, device, half=None):
            here = lambda: self.part(xx, yy, k, half)
            send((lambda: self.own) if source else here, here, sid(self.name + way), device)
            self.sends.append(pending.pop())

        def first_x(self):
            self.to("x", True, x, y, at_x)

        def first_y(self):
            self.to("y", True, x, y, at_y)

        def first_k(self):
            self.to("k0", True, x, y, at_k)

        def got_x(self):
            arrived(self.part(ox, y, k, None), sid(self.name + "x"))
            self.to("ya", False, ox, y, at_y, 0 if self.both else None)
            self.to("k1", False, ox, y, at_k)

        def got_y(self):
            arrived(self.part(x, oy, k, None), sid(self.name + "y"))
            if self.both:
                self.to("xb", False, x, oy, at_x, 1)
            self.to("k2", False, x, oy, at_k)

        def got_ya(self):
            half = 0 if self.both else None
            arrived(self.part(ox, oy, k, half), sid(self.name + "ya"))
            self.to("k3a", False, ox, oy, at_k, half)

        def got_xb(self):
            arrived(self.part(ox, oy, k, 1), sid(self.name + "xb"))
            self.to("k3b", False, ox, oy, at_k, 1)

        def near(self):
            self.copy.wait()
            for way, xx in (("k0", x), ("k1", ox)):
                arrived(self.part(xx, y, ok, None), sid(self.name + way))

        def whole(self):
            arrived(self.part(x, oy, ok, None), sid(self.name + "k2"))
            for half, way in ((0, "k3a"), (1, "k3b")) if self.both else ((None, "k3a"),):
                arrived(self.part(ox, oy, ok, half), sid(self.name + way))

    ex = Rows("ex", earlier_in, earlier_x, False)
    ct = Rows("ct", cot_in, cot_x, False)
    lx = Rows("lx", later_in, later_x, False)
    own_cols = lambda xx, c: up_in.at[:, span(xx * width + c * cw, cw)]
    own_rows = lambda xx, c: down_in.at[span(xx * width + c * cw, cw), :]
    up_a = [Line("uA", c, x, up_block, lambda c=c: own_cols(x, c)) for c in range(chunks)]
    up_b = [Line("uB", c, ox, up_block) for c in range(chunks)]
    down_a = [Line("dA", c, x, down_block, lambda c=c: own_rows(x, c)) for c in range(chunks)]
    down_b = [Line("dB", c, ox, down_block) for c in range(chunks)]
    copies = []
    for c in range(chunks):
        for source, dest, name in (
            (own_cols(x, c), up_block(z, x, c), "u"),
            (own_rows(x, c), down_block(z, x, c), "d"),
        ):
            copies.append(
                pltpu.make_async_copy(source, dest, local_sem.at[lid(f"local {name}{c}")])
            )

    def swap_up(c):
        send(lambda: own_cols(ox, c), lambda: up_block(z, x, c), sid(f"ux{c}"), at_x)

    def swap_down(c):
        send(lambda: own_rows(ox, c), lambda: down_block(z, x, c), sid(f"dx{c}"), at_x)

    def swapped_up(c):
        arrived(up_block(z, ox, c), sid(f"ux{c}"))
        up_b[c].first()

    def swapped_down(c):
        arrived(down_block(z, ox, c), sid(f"dx{c}"))
        down_b[c].first()

    def dot(a, b, dims):
        return lax.dot_general(a, b, (dims, ((), ())), preferred_element_type=jnp.float32)

    row_tiles = 2 * tokens // tile

    def gate_chunk(j):
        @pl.loop(0, row_tiles)
        def _(i):
            rows, cols = span(i * tile, tile), span(j * cw, cw)
            value = jnp.maximum(dot(earlier_x[rows, :], up_w[:, cols], ((1,), (0,))), 0.0)
            gate[rows, cols] = value.astype(jnp.bfloat16)
            squared[rows, :] = (value * value).astype(jnp.bfloat16)

    def later_chunk(j, place):
        cols = span(j * cw, cw)

        @pl.loop(0, row_tiles)
        def _(i):
            rows = span(i * tile, tile)
            value = dot(later_x[rows, :], up_w[:, cols], ((1,), (0,)))
            place[rows, :] = value.astype(jnp.bfloat16)
            value = jnp.maximum(value, 0.0)
            hidden[rows, cols] = (value * value).astype(jnp.bfloat16)

        out_cols = span(x * width + j * cw, cw)
        send(
            lambda: place.at[span(ox * tokens, tokens), :],
            lambda: preact_out.at[:, out_cols],
            sid(f"pre{j}"),
            at_x,
        )
        copy = pltpu.make_async_copy(
            place.at[span(x * tokens, tokens), :],
            preact_out.at[:, out_cols],
            local_sem.at[lid(f"local pre{j}")],
        )
        copy.start()
        return copy

    def slope_chunk(j):
        @pl.loop(0, row_tiles)
        def _(i):
            rows, cols = span(i * tile, tile), span(j * cw, cw)
            value = dot(cot_x[rows, :], down_w[cols, :], ((1,), (1,)))
            value = 2.0 * gate[rows, cols].astype(jnp.float32) * value
            gate[rows, cols] = value.astype(jnp.bfloat16)

    class Sum:
        def __init__(self, name, left, terms, got, out, run, place):
            self.name, self.left, self.terms, self.got, self.out = name, left, terms, got, out
            self.run, self.place, self.stores = run, place, {}

        def rows(self, o, q):
            return span(o * slab + (ox, x)[q] * fan, fan)

        def part(self, o, j, q):
            return self.terms.at[self.rows(o, q), span(j * cw, cw)]

        def slot(self, s, j, q):
            return self.got.at[s, span(q * fan, fan), span(j * cw, cw)]

        def owner(self, s):
            near = y * 2 >= nz // 2
            up_first = jnp.where(near, top - s, (nz // 2 - 1 - s) % nz)
            down_first = jnp.where(near, (nz // 2 + s) % nz, s)
            return jnp.where(z * 2 < nz, up_first, down_first)

        def compute(self, j, right, places):
            for s in places:
                o = self.owner(s)
                for q in range(2):
                    self.piece(o, j, q, right)
                    self.push(o, j, q, 1, (z == 0) & (o > 0))
                    self.push(o, j, q, -1, (z == top) & (o < top))

        def piece(self, o, j, q, right):
            value = dot(self.left[:, self.rows(o, q)], right(), ((0,), (0,)))
            self.terms[self.rows(o, q), span(j * cw, cw)] = value.astype(jnp.bfloat16)

        def push(self, o, j, q, way, when):
            base = sid(f"{self.name}{j}{q}", 2 * top)
            index, s, device = (base + o - 1, o + 1, at_up) if way > 0 else (base + top + o, o, at_down)
            send(lambda: self.part(o, j, q), lambda: self.slot(s, j, q), index, device, when)

        def add(self, o, s, j, q):
            value = self.part(o, j, q)[...].astype(jnp.float32)
            value = value + self.slot(s, j, q)[...].astype(jnp.float32)
            self.terms[self.rows(o, q), span(j * cw, cw)] = value.astype(jnp.bfloat16)

        def step(self, t, j, q):
            base = sid(f"{self.name}{j}{q}", 2 * top)
            up = top - t + z
            down = z - (top - t)

            @pl.when((z >= 1) & (t >= z))
            def _():
                arrived(self.slot(up + 1, j, q), base + up - 1)
                self.add(up, up + 1, j, q)

            if t < top:
                self.push(up, j, q, 1, (z >= 1) & (t >= z))

            @pl.when((z < top) & (t >= top - z))
            def _():
                arrived(self.slot(down, j, q), base + top + down)
                self.add(down, down, j, q)

            if t < top:
                self.push(down, j, q, -1, (z < top) & (t >= top - z))
                return
            if q == 0:
                send(
                    lambda: self.part(z, j, 0),
                    lambda: swap_got.at[self.place + j],
                    sid(f"{self.name}x{j}"),
                    at_x,
                )

        def loading(self, h, j):
            cols = span((x, ox)[h] * width + j * cw, cw)
            name = f"local {self.name} load {h}{j}"
            return pltpu.make_async_copy(
                self.run.at[:, cols], running.at[2 * h + j], local_sem.at[lid(name)]
            )

        def load(self, h, j):
            self.loading(h, j).start()

        def store(self, h, j, value):
            self.loading(h, j).wait()
            running[2 * h + j] = running[2 * h + j] + value.astype(jnp.float32) * factor
            cols = span((x, ox)[h] * width + j * cw, cw)
            name = f"local {self.name} store {h}{j}"
            copy = pltpu.make_async_copy(
                running.at[2 * h + j], self.out.at[:, cols], local_sem.at[lid(name)]
            )
            copy.start()
            self.stores[h, j] = copy

        def own(self, j):
            self.store(0, j, self.part(z, j, 1)[...])

        def other(self, j):
            arrived(swap_got.at[self.place + j], sid(f"{self.name}x{j}"))
            self.store(1, j, swap_got[self.place + j])

    def next_load(h, j):
        down_sum.stores[h, j].wait()
        up_sum.load(h, j)

    class Partial:
        def __init__(self, name, left, right, dims, total, got, last, out, both):
            self.both = both
            self.name, self.left, self.right, self.dims = name, left, right, dims
            self.total, self.got, self.last, self.out = total, got, last, out

        def rows(self, h):
            return ox if h == 0 else x

        def tile_of(self, h, yy, kk):
            return self.total.at[
                span(self.rows(h) * tokens, tokens), span((yy * 2 + kk) * feats, feats)
            ]

        def half_of(self, h, yy, half):
            if half is None:
                return self.tile_of(h, yy, k)
            cols = span((yy * 2 + k) * feats + half * (feats // 2), feats // 2)
            return self.total.at[span(self.rows(h) * tokens, tokens), cols]

        def slot(self, h, c):
            return self.got.at[span(h * tokens, tokens), span(c * feats, feats)]

        def half_slot(self, way):
            if not self.both:
                return self.last if way == "x3" else self.slot(int(way[1]) - 1, 2)
            n = ("y1", "y2", "y3", "x1", "x2", "x3").index(way)
            if n < 4:
                cols = span(2 * feats + (n % 2) * (feats // 2), feats // 2)
                return self.got.at[span((n // 2) * tokens, tokens), cols]
            return self.last.at[:, span((n % 2) * (feats // 2), feats // 2)]

        def columns(self, h, kk):
            for yy in range(2):
                cols = span((yy * 2 + kk) * feats, feats)

                @pl.loop(0, tokens // tile)
                def _(i):
                    rows = span(self.rows(h) * tokens + i * tile, tile)
                    right = self.right[cols, :] if self.dims == ((1,), (1,)) else self.right[:, cols]
                    value = dot(self.left[rows, :], right, self.dims)
                    self.total[rows, cols] = value.astype(jnp.bfloat16)

        def compute(self, h):
            self.columns(h, ok)
            for yy in range(2):
                send(
                    lambda yy=yy: self.tile_of(h, yy, ok),
                    lambda yy=yy: self.slot(h, yy),
                    sid(f"{self.name}k{h}{yy}"),
                    at_k,
                )
            self.columns(h, k)

        def add(self, mine, got):
            @pl.loop(0, tokens // tile)
            def _(i):
                rows = span(i * tile, tile)
                value = mine[rows, :].astype(jnp.float32) + got[rows, :].astype(jnp.float32)
                mine[rows, :] = value.astype(jnp.bfloat16)

        def pass_on(self, way, h, yy, half):
            send(
                lambda: self.half_of(h, yy, half),
                lambda: self.half_slot(way),
                sid(self.name + way),
                at_y if way[0] == "y" else at_x,
            )

        def take(self, way, h, yy, half):
            arrived(self.half_slot(way), sid(self.name + way))
            self.add(self.half_of(h, yy, half), self.half_slot(way))

        def after_k(self, h):
            for yy in range(2):
                arrived(self.slot(h, yy), sid(f"{self.name}k{h}{yy}"))
            self.add(self.tile_of(h, oy, k), self.slot(h, oy))
            half = 0 if self.both else None
            self.pass_on(f"y{h + 1}", h, oy, half)
            if h == 0 and self.both:
                self.pass_on("x1", 0, oy, 1)
            self.add(self.tile_of(h, y, k), self.slot(h, y))
            if h == 0 and self.both:
                self.pass_on("x2", 0, y, 1)

        def second(self):
            half = None
            if self.both:
                half = 0
                self.take("x1", 1, oy, 1)
                self.pass_on("y3", 1, oy, 1)
            self.take("y1", 0, y, half)
            self.pass_on("x3", 0, y, half)

        def finish(self):
            if self.both:
                self.take("x2", 1, y, 1)
                self.take("y3", 1, y, 1)
            half = 0 if self.both else None
            self.take("y2", 1, y, half)
            self.take("x3", 1, y, half)
            copy = pltpu.make_async_copy(
                self.tile_of(1, y, k), self.out, local_sem.at[lid(f"local {self.name}")]
            )
            copy.start()
            locals_.append(copy)

    locals_ = []
    down_sum = Sum("ds", cot_x, down_terms, down_got, down_out, down_run, 0)
    up_sum = Sum("us", earlier_x, up_terms, up_got, up_out, up_run, chunks)
    cols_of = lambda j: span(j * cw, cw)

    product = Partial("po", hidden, down_w, ((1,), (0,)), later_x, parts_got, last_got, later_out, True)
    back = Partial(
        "pb",
        gate,
        up_w,
        ((1,), (1,)),
        cot_x,
        earlier_x,
        earlier_x.at[span(0, tokens), span(3 * feats, feats)],
        grad_out,
        False,
    )
    def settle_later():
        for entry in lx.sends:
            sent(entry)

    def settle_cot():
        for entry in ct.sends:
            sent(entry)

    def settle_earlier():
        for entry in ex.sends:
            sent(entry)
        for device in (at_x, at_y, at_k):
            pl.semaphore_signal(ready_sem, inc=1, device_id=device, device_id_type=MESH)

    def others_ready():
        pl.semaphore_wait(ready_sem, 3)

    later_copies = []
    up_a[0].first()
    ex.first_y()
    swap_up(0)
    ex.first_k()
    ct.first_k()
    swap_up(1)
    down_a[0].first()
    ct.first_y()
    down_sum.load(1, 1)
    ex.first_x()
    for copy in copies:
        copy.start()
    ex.local()
    ct.local()
    lx.local()
    swapped_up(0)
    ct.first_x()
    up_a[0].inner(1)
    lx.first_k()
    swapped_up(1)
    up_a[1].first()
    ex.got_y()
    up_a[0].outer(1)
    swap_down(0)
    down_sum.load(0, 1)
    up_b[0].outer(1)
    up_b[1].outer(1)
    down_a[1].first()
    ex.got_x()
    swap_down(1)
    up_b[0].inner(1)
    ct.got_y()
    up_a[0].inner(2)
    lx.first_x()
    up_a[1].outer(1)
    ct.got_x()
    up_b[0].inner(2)
    up_a[0].inner(3)
    up_a[1].inner(1)
    ex.got_ya()
    ct.near()
    ex.near()
    up_b[1].inner(1)
    swapped_down(0)
    up_b[0].inner(3)
    down_sum.load(0, 0)
    swapped_down(1)
    down_a[0].outer(1)
    lx.first_y()
    ex.whole()
    for copy in copies:
        copy.wait()
    gate_chunk(0)
    down_b[0].outer(1)
    down_sum.compute(0, lambda: squared[...], (0, 1))
    ct.got_ya()
    down_a[1].outer(1)
    up_b[1].inner(2)
    ct.whole()
    down_sum.compute(0, lambda: squared[...], (2, 3))
    up_a[1].inner(2)
    down_b[1].outer(1)
    lx.got_x()
    down_b[0].inner(1)
    up_a[1].inner(3)
    lx.near()
    lx.got_y()
    down_b[1].inner(1)
    up_b[1].inner(3)
    down_a[1].inner(1)
    gate_chunk(1)
    down_sum.compute(1, lambda: squared[...], (0, 1))
    down_sum.step(1, 0, 1)
    down_sum.step(1, 0, 0)
    down_sum.compute(1, lambda: squared[...], (2, 3))
    lx.got_ya()
    down_a[0].inner(1)
    lx.whole()
    later_copies.append(later_chunk(0, staged))
    down_a[1].inner(2)
    down_b[1].inner(2)
    down_a[1].inner(3)
    later_copies.append(later_chunk(1, squared))
    down_b[0].inner(2)
    down_a[0].inner(2)
    down_b[1].inner(3)
    down_sum.step(2, 0, 0)
    settle_later()
    slope_chunk(1)
    down_sum.step(1, 1, 0)
    down_sum.step(2, 0, 1)
    up_sum.compute(1, lambda: gate[:, cols_of(1)], range(nz))
    down_a[0].inner(3)
    down_b[0].inner(3)
    down_sum.step(1, 1, 1)
    product.compute(0)
    down_sum.step(3, 0, 0)
    product.compute(1)
    product.after_k(0)
    down_sum.load(1, 0)
    down_sum.step(2, 1, 0)
    slope_chunk(0)
    down_sum.step(2, 1, 1)
    up_sum.compute(0, lambda: gate[:, cols_of(0)], range(nz))
    settle_earlier()
    settle_cot()
    product.after_k(1)
    up_sum.step(1, 1, 0)
    down_sum.step(3, 1, 0)
    down_sum.step(3, 0, 1)
    others_ready()
    back.compute(0)
    up_sum.step(1, 1, 1)
    back.after_k(0)
    up_sum.step(2, 1, 0)
    down_sum.step(3, 1, 1)
    product.second()
    up_sum.step(2, 1, 1)
    back.compute(1)
    up_sum.step(3, 1, 0)
    down_sum.own(0)
    back.after_k(1)
    up_sum.step(1, 0, 0)
    back.second()
    down_sum.own(1)
    next_load(0, 0)
    up_sum.step(1, 0, 1)
    down_sum.other(1)
    up_sum.step(2, 0, 0)
    up_sum.step(2, 0, 1)
    up_sum.step(3, 1, 1)
    next_load(1, 1)
    up_sum.other(1)
    down_sum.other(0)
    up_sum.step(3, 0, 0)
    up_sum.step(3, 0, 1)
    next_load(1, 0)
    up_sum.own(0)
    product.finish()
    next_load(0, 1)
    up_sum.own(1)
    up_sum.other(0)
    back.finish()
    for j in range(chunks):
        arrived(preact_out.at[:, span(ox * width + j * cw, cw)], sid(f"pre{j}"))
    for copy in later_copies + locals_ + list(up_sum.stores.values()):
        copy.wait()
    for entry in pending:
        sent(entry)


def on_device_rings(
    later_input, earlier_input, cotangent, up_weight, down_weight, up_running, down_running
):
    n = lax.axis_size("fs")
    factor = float(later_input.shape[0] * n) ** (-0.5)

    up_full, up_arrived = ring_gather(up_weight)
    inputs = tp_gather(jnp.stack((later_input, earlier_input, cotangent)))
    later_full, earlier_full, cot_full = inputs[0], inputs[1], inputs[2]
    down_rows = after(down_weight.T, inputs, *up_arrived[-4])
    down_full, down_arrived = ring_gather(down_rows)

    earlier_up = jnp.dot(earlier_full, up_full, preferred_element_type=jnp.float32)
    earlier_relu = jax.nn.relu(earlier_up)
    earlier_hidden = jnp.square(earlier_relu).astype(jnp.bfloat16)
    down_terms = lax.dot_general(
        cot_full, earlier_hidden, contract_first, preferred_element_type=jnp.float32
    ).astype(jnp.bfloat16)
    down_sum = ring_scatter(down_terms, down_arrived[-4])

    later_up = jnp.dot(later_full, up_full, preferred_element_type=jnp.float32)
    later_preact = later_up.astype(jnp.bfloat16)
    later_hidden = jnp.square(jax.nn.relu(later_up)).astype(jnp.bfloat16)

    grad = jnp.dot(cot_full, down_full, preferred_element_type=jnp.float32)
    up_grad = (2.0 * earlier_relu * grad).astype(jnp.bfloat16)
    up_terms = lax.dot_general(
        earlier_full, up_grad, contract_first, preferred_element_type=jnp.float32
    ).astype(jnp.bfloat16)
    up_sum = ring_scatter(up_terms)

    back_part = lax.dot_general(
        up_grad, up_full, contract_last, preferred_element_type=jnp.float32
    ).astype(jnp.bfloat16)
    product = lax.dot_general(
        later_hidden, down_full, contract_last, preferred_element_type=jnp.float32
    ).astype(jnp.bfloat16)
    return (
        tp_scatter(product),
        later_preact,
        tp_scatter(back_part),
        up_running + up_sum * factor,
        down_running + down_sum * factor,
    )


def across_x(n_fs):
    return 1 << ((n_fs.bit_length() - 1) // 2)


def hand_over_kernel(pieces, count, *refs):
    sources, targets, held = refs[:count], refs[count : 2 * count], refs[2 * count : 3 * count]
    in_sem, out_sem = refs[3 * count :]
    reads, writes = [], []
    for n, rows, size in pieces:
        part, index = pl.ds(rows, size), len(reads)
        here = held[n].at[part, :]
        reads.append(pltpu.make_async_copy(sources[n].at[part, :], here, in_sem.at[index]))
        writes.append(pltpu.make_async_copy(here, targets[n].at[part, :], out_sem.at[index]))
    for read in reads:
        read.start()
    for read, write in zip(reads, writes):
        read.wait()
        write.start()
    for write in writes:
        write.wait()


def hand_over(arrays):
    pieces = []
    for n, array in enumerate(arrays):
        size = max(array.shape[0] * MIB // (array.size * array.dtype.itemsize), 1)
        size = math.gcd(array.shape[0], 1 << (size.bit_length() - 1))
        pieces += [(n, rows, size) for rows in range(0, array.shape[0], size)]
    in_hbm = pl.BlockSpec(memory_space=pltpu.HBM)
    return pl.pallas_call(
        functools.partial(hand_over_kernel, pieces, len(arrays)),
        out_shape=tuple(jax.ShapeDtypeStruct(a.shape, a.dtype) for a in arrays),
        in_specs=[in_hbm] * len(arrays),
        out_specs=(in_hbm,) * len(arrays),
        scratch_shapes=[pltpu.VMEM(a.shape, a.dtype) for a in arrays]
        + [pltpu.SemaphoreType.DMA((len(pieces),))] * 2,
        compiler_params=pltpu.CompilerParams(vmem_limit_bytes=VMEM_BYTES),
        name="hand_over",
    )(*arrays)


def on_device_kernel(
    later_input, earlier_input, cotangent, up_weight, down_weight, up_running, down_running
):
    n = lax.axis_size("fs")
    nz = n // 2
    tokens, feats = later_input.shape
    fan, width = up_weight.shape[0], up_weight.shape[1] // 2
    depth, rows = n * fan, 2 * tokens
    factor = float(tokens * n) ** (-0.5)
    bf16 = jnp.bfloat16
    semaphores = 32 * (nz - 1) + 48
    anywhere = pl.BlockSpec(memory_space=pl.ANY)
    outputs = pl.pallas_call(
        functools.partial(layer_kernel, nz, factor),
        out_shape=(
            jax.ShapeDtypeStruct((tokens, feats), bf16),
            jax.ShapeDtypeStruct((tokens, 2 * width), bf16),
            jax.ShapeDtypeStruct((tokens, feats), bf16),
            jax.ShapeDtypeStruct((fan, 2 * width), jnp.float32),
            jax.ShapeDtypeStruct((fan, 2 * width), jnp.float32),
        ),
        in_specs=[anywhere] * 7,
        out_specs=(anywhere,) * 5,
        scratch_shapes=[
            pltpu.VMEM((rows, depth), bf16),
            pltpu.VMEM((rows, depth), bf16),
            pltpu.VMEM((rows, depth), bf16),
            pltpu.VMEM((depth, width), bf16),
            pltpu.VMEM((width, depth), bf16),
            pltpu.VMEM((rows, width), bf16),
            pltpu.VMEM((rows, width), bf16),
            pltpu.VMEM((rows, width // 2), bf16),
            pltpu.VMEM((rows, width // 2), bf16),
            pltpu.VMEM((depth, width), bf16),
            pltpu.VMEM((depth, width), bf16),
            pltpu.VMEM((nz + 1, 2 * fan, width), bf16),
            pltpu.VMEM((nz + 1, 2 * fan, width), bf16),
            pltpu.VMEM((rows, 3 * feats), bf16),
            pltpu.VMEM((tokens, feats), bf16),
            pltpu.VMEM((4, fan, width // 2), bf16),
            pltpu.VMEM((4, fan, width // 2), jnp.float32),
            pltpu.SemaphoreType.DMA((semaphores,)),
            pltpu.SemaphoreType.DMA((semaphores,)),
            pltpu.SemaphoreType.DMA((27,)),
            pltpu.SemaphoreType.REGULAR,
        ],
        compiler_params=pltpu.CompilerParams(
            collective_id=0, has_side_effects=True, vmem_limit_bytes=VMEM_BYTES
        ),
        name="layer",
    )(later_input, earlier_input, cotangent, up_weight, down_weight, up_running, down_running)
    return hand_over(outputs)


def on_device(*arrays):
    square = across_x(lax.axis_size("fs")) == 2 and lax.axis_size("tp") == 4
    return (on_device_kernel if square else on_device_rings)(*arrays)


def solution(mesh):
    in_specs = (
        P("fs", "tp"),
        P("fs", "tp"),
        P("fs", "tp"),
        P("fs", "tp"),
        P("tp", "fs"),
        P("fs", "tp"),
        P("fs", "tp"),
    )
    out_specs = (P("fs", "tp"), P("fs", "tp"), P("fs", "tp"), P("fs", "tp"), P("fs", "tp"))
    return jax.shard_map(
        on_device, mesh=mesh, in_specs=in_specs, out_specs=out_specs, check_vma=False
    )
```

```python
import functools
import math

import jax
import jax.numpy as jnp
from jax import lax
from jax.experimental import pallas as pl
from jax.experimental.pallas import tpu as pltpu
from jax.sharding import PartitionSpec as P

contract_last = (((1,), (1,)), ((), ()))
contract_first = (((0,), (0,)), ((), ()))


STREAMS = 4


def ring_index(place, n):
    place = lax.rem(place + 2 * n, n)
    return jnp.where(place < n // 2, 2 * place, 2 * (n - place) - 1)


def ring_pairs(n, direction):
    order = [q * 2 if q < n // 2 else 2 * (n - q) - 1 for q in range(n)]
    return [(order[q], order[(q + direction) % n]) for q in range(n)]


def my_place(n):
    me = lax.axis_index("fs")
    half = lax.div(me, 2)
    return jnp.where(lax.rem(me, 2) == 0, half, n - 1 - half)


def after(value, *others):
    return lax.optimization_barrier((value, *others))[0]


def ring_gather(shard):
    n = lax.axis_size("fs")
    rows, columns = shard.shape
    place = my_place(n)
    blocks = shard.reshape(STREAMS, rows // STREAMS, columns)
    held = [blocks[s : s + 1] for s in range(STREAMS)]
    full = jnp.zeros((n, STREAMS, rows // STREAMS, columns), shard.dtype)
    full = lax.dynamic_update_slice(full, blocks[None], (lax.axis_index("fs"), 0, 0, 0))
    arrived = []
    for step in range(1, n):
        for s in range(STREAMS):
            direction = 1 if s % 2 == 0 else -1
            held[s] = lax.ppermute(held[s], "fs", ring_pairs(n, direction))
            owner = ring_index(place - direction * step, n)
            full = lax.dynamic_update_slice(full, held[s][None], (owner, s, 0, 0))
        arrived.append(tuple(held))
    return full.reshape(n * rows, columns), arrived


def ring_scatter(terms, wait_for=()):
    n = lax.axis_size("fs")
    rows, columns = terms.shape[0] // n, terms.shape[1]
    place = my_place(n)
    blocks = terms.reshape(n, STREAMS, rows // STREAMS, columns)

    def own(s, direction, step):
        owner = ring_index(place - direction * (step + 1), n)
        return lax.dynamic_slice(
            blocks, (owner, s, 0, 0), (1, 1, rows // STREAMS, columns)
        ).reshape(rows // STREAMS, columns)

    totals = [own(s, 1 if s % 2 == 0 else -1, 0) for s in range(STREAMS)]
    if wait_for:
        totals = [after(total, *wait_for) for total in totals]
    for step in range(1, n):
        for s in range(STREAMS):
            direction = 1 if s % 2 == 0 else -1
            got = lax.ppermute(
                totals[s].astype(jnp.bfloat16), "fs", ring_pairs(n, direction)
            )
            totals[s] = got.astype(jnp.float32) + own(s, direction, step).astype(jnp.float32)
    return jnp.concatenate(totals, axis=0)


def flip_pairs(n, mask):
    return [(i, i ^ mask) for i in range(n)]


def tp_gather(block):
    n = lax.axis_size("tp")
    me = lax.axis_index("tp")
    blocks = [block]
    mask = n // 2
    while mask:
        upper = (me & mask) != 0
        merged = []
        for mine in blocks:
            other = lax.ppermute(mine, "tp", flip_pairs(n, mask))
            merged += [jnp.where(upper, other, mine), jnp.where(upper, mine, other)]
        blocks = merged
        mask //= 2
    return jnp.concatenate(blocks, axis=-1)


def tp_scatter(terms):
    n = lax.axis_size("tp")
    me = lax.axis_index("tp")
    width = terms.shape[1] // n
    blocks = [terms[:, j * width : (j + 1) * width] for j in range(n)]
    mask = 1
    while mask < n:
        upper = (me & mask) != 0
        kept = []
        for low, high in zip(blocks[0::2], blocks[1::2]):
            sent = jnp.where(upper, low, high).astype(jnp.bfloat16)
            mine = jnp.where(upper, high, low)
            got = lax.ppermute(sent, "tp", flip_pairs(n, mask))
            kept.append(mine.astype(jnp.float32) + got.astype(jnp.float32))
        blocks = kept
        mask *= 2
    return blocks[0].astype(jnp.bfloat16)


MESH = pl.DeviceIdType.MESH
VMEM_BYTES = 67043328
MIB = 1 << 20


def span(start, size):
    if not isinstance(start, int):
        start = pl.multiple_of(start, size)
    return pl.ds(start, size)


def layer_kernel(
    nz,
    factor,
    later_in,
    earlier_in,
    cot_in,
    up_in,
    down_in,
    up_run,
    down_run,
    later_out,
    preact_out,
    grad_out,
    up_out,
    down_out,
    later_x,
    earlier_x,
    cot_x,
    up_w,
    down_w,
    gate,
    hidden,
    squared,
    staged,
    down_terms,
    up_terms,
    down_got,
    up_got,
    parts_got,
    last_got,
    swap_got,
    running,
    send_sem,
    recv_sem,
    local_sem,
    ready_sem,
):
    fs, tp = lax.axis_index("fs"), lax.axis_index("tp")
    z, x = lax.div(fs, 2), lax.rem(fs, 2)
    y, k = lax.div(tp, 2), lax.rem(tp, 2)
    ox, oy, ok = 1 - x, 1 - y, 1 - k
    at_x, at_y, at_k = (z * 2 + ox, tp), (fs, oy * 2 + k), (fs, y * 2 + ok)
    at_up, at_down = (fs + 2, tp), (fs - 2, tp)
    top = nz - 1

    tokens, feats = later_in.shape
    fan = up_in.shape[0]
    width = up_w.shape[1]
    slab = 2 * fan
    chunks = 2
    cw = width // chunks
    tile = math.gcd(tokens, slab)

    ids, local_ids = {}, {}
    pending = []

    def sid(name, count=1):
        if name not in ids:
            ids[name] = sum(c for _, c in ids.values()), count
        return ids[name][0]

    def lid(name):
        return local_ids.setdefault(name, len(local_ids))

    def remote(src, dst, index, device):
        return pltpu.make_async_remote_copy(
            src_ref=src,
            dst_ref=dst,
            send_sem=send_sem.at[index],
            recv_sem=recv_sem.at[index],
            device_id=device,
            device_id_type=MESH,
        )

    def send(src, dst, index, device, when=None):
        def go():
            remote(src(), dst(), index, device).start()

        if when is None:
            go()
        else:
            pl.when(when)(go)
        pending.append((src, dst, index, device, when))

    def sent(entry):
        src, dst, index, device, when = entry

        def go():
            remote(src(), dst(), index, device).wait_send()

        if when is None:
            go()
        else:
            pl.when(when)(go)

    def arrived(dst, index):
        remote(dst, dst, index, at_x).wait_recv()

    barrier = pltpu.get_barrier_semaphore()
    for device in (at_x, at_y, at_k):
        pl.semaphore_signal(barrier, inc=1, device_id=device, device_id_type=MESH)

    @pl.when(z > 0)
    def _():
        pl.semaphore_signal(barrier, inc=1, device_id=at_down, device_id_type=MESH)

    @pl.when(z < top)
    def _():
        pl.semaphore_signal(barrier, inc=1, device_id=at_up, device_id_type=MESH)

    pl.semaphore_wait(barrier, 3 + jnp.where(z > 0, 1, 0) + jnp.where(z < top, 1, 0))

    def block(ref, xx, yy, kk):
        return ref.at[span(xx * tokens, tokens), span((yy * 2 + kk) * feats, feats)]

    def up_block(zz, xx, c):
        return up_w.at[span((zz * 2 + xx) * fan, fan), span(c * cw, cw)]

    def down_block(zz, xx, c):
        return down_w.at[span(c * cw, cw), span((zz * 2 + xx) * fan, fan)]

    class Line:
        def __init__(self, name, c, xx, place, own=None):
            self.base = sid(f"{name}{c}", 2 * top)
            self.place = lambda zz: place(zz, xx, c)
            self.own = own or (lambda: self.place(z))

        def first(self):
            here = lambda: self.place(z)
            send(self.own, here, self.base, at_up, z < top)
            send(self.own, here, self.base + top, at_down, z > 0)

        def inner(self, h):
            low, high = z * 2 < nz, z * 2 >= nz

            @pl.when(high & (z >= h))
            def _():
                arrived(self.place(z - h), self.base + h - 1)

            @pl.when(low & (z + h <= top))
            def _():
                arrived(self.place(z + h), self.base + top + h - 1)

            if h < top:
                here, there = lambda: self.place(z - h), lambda: self.place(z + h)
                send(here, here, self.base + h, at_up, high & (z >= h) & (z < top))
                send(there, there, self.base + top + h, at_down, low & (z + h <= top) & (z > 0))

        def outer(self, h):
            low, high = z * 2 < nz, z * 2 >= nz
            here, there = lambda: self.place(z - h), lambda: self.place(z + h)

            @pl.when(low & (z >= h))
            def _():
                arrived(self.place(z - h), self.base + h - 1)

            send(here, here, self.base + h, at_up, low & (z >= h))

            @pl.when(high & (z + h <= top))
            def _():
                arrived(self.place(z + h), self.base + top + h - 1)

            send(there, there, self.base + top + h, at_down, high & (z + h <= top))

    class Rows:
        def __init__(self, name, own, full, both):
            self.name, self.own, self.full, self.both, self.sends = name, own, full, both, []
            self.copy = pltpu.make_async_copy(own, block(full, x, y, k), local_sem.at[lid("local " + name)])

        def local(self):
            self.copy.start()

        def part(self, xx, yy, kk, half):
            if half is None:
                return block(self.full, xx, yy, kk)
            cols = span((yy * 2 + kk) * feats + half * (feats // 2), feats // 2)
            return self.full.at[span(xx * tokens, tokens), cols]

        def to(self, way, source, xx, yy, device, half=None):
            here = lambda: self.part(xx, yy, k, half)
            send((lambda: self.own) if source else here, here, sid(self.name + way), device)
            self.sends.append(pending.pop())

        def first_x(self):
            self.to("x", True, x, y, at_x)

        def first_y(self):
            self.to("y", True, x, y, at_y)

        def first_k(self):
            self.to("k0", True, x, y, at_k)

        def got_x(self):
            arrived(self.part(ox, y, k, None), sid(self.name + "x"))
            self.to("ya", False, ox, y, at_y, 0 if self.both else None)
            self.to("k1", False, ox, y, at_k)

        def got_y(self):
            arrived(self.part(x, oy, k, None), sid(self.name + "y"))
            if self.both:
                self.to("xb", False, x, oy, at_x, 1)
            self.to("k2", False, x, oy, at_k)

        def got_ya(self):
            half = 0 if self.both else None
            arrived(self.part(ox, oy, k, half), sid(self.name + "ya"))
            self.to("k3a", False, ox, oy, at_k, half)

        def got_xb(self):
            arrived(self.part(ox, oy, k, 1), sid(self.name + "xb"))
            self.to("k3b", False, ox, oy, at_k, 1)

        def near(self):
            self.copy.wait()
            for way, xx in (("k0", x), ("k1", ox)):
                arrived(self.part(xx, y, ok, None), sid(self.name + way))

        def whole(self):
            arrived(self.part(x, oy, ok, None), sid(self.name + "k2"))
            for half, way in ((0, "k3a"), (1, "k3b")) if self.both else ((None, "k3a"),):
                arrived(self.part(ox, oy, ok, half), sid(self.name + way))

    ex = Rows("ex", earlier_in, earlier_x, False)
    ct = Rows("ct", cot_in, cot_x, False)
    lx = Rows("lx", later_in, later_x, True)
    own_cols = lambda xx, c: up_in.at[:, span(xx * width + c * cw, cw)]
    own_rows = lambda xx, c: down_in.at[span(xx * width + c * cw, cw), :]
    up_a = [Line("uA", c, x, up_block, lambda c=c: own_cols(x, c)) for c in range(chunks)]
    up_b = [Line("uB", c, ox, up_block) for c in range(chunks)]
    down_a = [Line("dA", c, x, down_block, lambda c=c: own_rows(x, c)) for c in range(chunks)]
    down_b = [Line("dB", c, ox, down_block) for c in range(chunks)]
    copies = []
    for c in range(chunks):
        for source, dest, name in (
            (own_cols(x, c), up_block(z, x, c), "u"),
            (own_rows(x, c), down_block(z, x, c), "d"),
        ):
            copies.append(
                pltpu.make_async_copy(source, dest, local_sem.at[lid(f"local {name}{c}")])
            )

    def swap_up(c):
        send(lambda: own_cols(ox, c), lambda: up_block(z, x, c), sid(f"ux{c}"), at_x)

    def swap_down(c):
        send(lambda: own_rows(ox, c), lambda: down_block(z, x, c), sid(f"dx{c}"), at_x)

    def swapped_up(c):
        arrived(up_block(z, ox, c), sid(f"ux{c}"))
        up_b[c].first()

    def swapped_down(c):
        arrived(down_block(z, ox, c), sid(f"dx{c}"))
        down_b[c].first()

    def dot(a, b, dims):
        return lax.dot_general(a, b, (dims, ((), ())), preferred_element_type=jnp.float32)

    row_tiles = 2 * tokens // tile

    def gate_chunk(j):
        @pl.loop(0, row_tiles)
        def _(i):
            rows, cols = span(i * tile, tile), span(j * cw, cw)
            value = jnp.maximum(dot(earlier_x[rows, :], up_w[:, cols], ((1,), (0,))), 0.0)
            gate[rows, cols] = value.astype(jnp.bfloat16)
            squared[rows, :] = (value * value).astype(jnp.bfloat16)

    def later_chunk(j, place):
        cols = span(j * cw, cw)

        @pl.loop(0, row_tiles)
        def _(i):
            rows = span(i * tile, tile)
            value = dot(later_x[rows, :], up_w[:, cols], ((1,), (0,)))
            place[rows, :] = value.astype(jnp.bfloat16)
            value = jnp.maximum(value, 0.0)
            hidden[rows, cols] = (value * value).astype(jnp.bfloat16)

        out_cols = span(x * width + j * cw, cw)
        send(
            lambda: place.at[span(ox * tokens, tokens), :],
            lambda: preact_out.at[:, out_cols],
            sid(f"pre{j}"),
            at_x,
        )
        copy = pltpu.make_async_copy(
            place.at[span(x * tokens, tokens), :],
            preact_out.at[:, out_cols],
            local_sem.at[lid(f"local pre{j}")],
        )
        copy.start()
        return copy

    def slope_chunk(j):
        @pl.loop(0, row_tiles)
        def _(i):
            rows, cols = span(i * tile, tile), span(j * cw, cw)
            value = dot(cot_x[rows, :], down_w[cols, :], ((1,), (1,)))
            value = 2.0 * gate[rows, cols].astype(jnp.float32) * value
            gate[rows, cols] = value.astype(jnp.bfloat16)

    class Sum:
        def __init__(self, name, left, terms, got, out, run, place):
            self.name, self.left, self.terms, self.got, self.out = name, left, terms, got, out
            self.run, self.place, self.stores = run, place, {}

        def rows(self, o, q):
            return span(o * slab + (ox, x)[q] * fan, fan)

        def part(self, o, j, q):
            return self.terms.at[self.rows(o, q), span(j * cw, cw)]

        def slot(self, s, j, q):
            return self.got.at[s, span(q * fan, fan), span(j * cw, cw)]

        def owner(self, s):
            near = y * 2 >= nz // 2
            up_first = jnp.where(near, top - s, (nz // 2 - 1 - s) % nz)
            down_first = jnp.where(near, (nz // 2 + s) % nz, s)
            return jnp.where(z * 2 < nz, up_first, down_first)

        def compute(self, j, right, places):
            for s in places:
                o = self.owner(s)
                for q in range(2):
                    self.piece(o, j, q, right)
                    self.push(o, j, q, 1, (z == 0) & (o > 0))
                    self.push(o, j, q, -1, (z == top) & (o < top))

        def piece(self, o, j, q, right):
            value = dot(self.left[:, self.rows(o, q)], right(), ((0,), (0,)))
            self.terms[self.rows(o, q), span(j * cw, cw)] = value.astype(jnp.bfloat16)

        def push(self, o, j, q, way, when):
            base = sid(f"{self.name}{j}{q}", 2 * top)
            index, s, device = (base + o - 1, o + 1, at_up) if way > 0 else (base + top + o, o, at_down)
            send(lambda: self.part(o, j, q), lambda: self.slot(s, j, q), index, device, when)

        def add(self, o, s, j, q):
            value = self.part(o, j, q)[...].astype(jnp.float32)
            value = value + self.slot(s, j, q)[...].astype(jnp.float32)
            self.terms[self.rows(o, q), span(j * cw, cw)] = value.astype(jnp.bfloat16)

        def step(self, t, j, q):
            base = sid(f"{self.name}{j}{q}", 2 * top)
            up = top - t + z
            down = z - (top - t)

            @pl.when((z >= 1) & (t >= z))
            def _():
                arrived(self.slot(up + 1, j, q), base + up - 1)
                self.add(up, up + 1, j, q)

            if t < top:
                self.push(up, j, q, 1, (z >= 1) & (t >= z))

            @pl.when((z < top) & (t >= top - z))
            def _():
                arrived(self.slot(down, j, q), base + top + down)
                self.add(down, down, j, q)

            if t < top:
                self.push(down, j, q, -1, (z < top) & (t >= top - z))
                return
            if q == 0:
                send(
                    lambda: self.part(z, j, 0),
                    lambda: swap_got.at[self.place + j],
                    sid(f"{self.name}x{j}"),
                    at_x,
                )

        def loading(self, h, j):
            cols = span((x, ox)[h] * width + j * cw, cw)
            name = f"local {self.name} load {h}{j}"
            return pltpu.make_async_copy(
                self.run.at[:, cols], running.at[2 * h + j], local_sem.at[lid(name)]
            )

        def load(self, h, j):
            self.loading(h, j).start()

        def store(self, h, j, value):
            self.loading(h, j).wait()
            running[2 * h + j] = running[2 * h + j] + value.astype(jnp.float32) * factor
            cols = span((x, ox)[h] * width + j * cw, cw)
            name = f"local {self.name} store {h}{j}"
            copy = pltpu.make_async_copy(
                running.at[2 * h + j], self.out.at[:, cols], local_sem.at[lid(name)]
            )
            copy.start()
            self.stores[h, j] = copy

        def own(self, j):
            self.store(0, j, self.part(z, j, 1)[...])

        def other(self, j):
            arrived(swap_got.at[self.place + j], sid(f"{self.name}x{j}"))
            self.store(1, j, swap_got[self.place + j])

    def next_load(h, j):
        down_sum.stores[h, j].wait()
        up_sum.load(h, j)

    class Partial:
        def __init__(self, name, left, right, dims, total, got, last, out, both):
            self.both = both
            self.name, self.left, self.right, self.dims = name, left, right, dims
            self.total, self.got, self.last, self.out = total, got, last, out

        def rows(self, h):
            return ox if h == 0 else x

        def tile_of(self, h, yy, kk):
            return self.total.at[
                span(self.rows(h) * tokens, tokens), span((yy * 2 + kk) * feats, feats)
            ]

        def half_of(self, h, yy, half):
            if half is None:
                return self.tile_of(h, yy, k)
            cols = span((yy * 2 + k) * feats + half * (feats // 2), feats // 2)
            return self.total.at[span(self.rows(h) * tokens, tokens), cols]

        def slot(self, h, c):
            return self.got.at[span(h * tokens, tokens), span(c * feats, feats)]

        def half_slot(self, way):
            if not self.both:
                return self.last if way == "x3" else self.slot(int(way[1]) - 1, 2)
            n = ("y1", "y2", "y3", "x1", "x2", "x3").index(way)
            if n < 4:
                cols = span(2 * feats + (n % 2) * (feats // 2), feats // 2)
                return self.got.at[span((n // 2) * tokens, tokens), cols]
            return self.last.at[:, span((n % 2) * (feats // 2), feats // 2)]

        def columns(self, h, yy, kk):
            cols = span((yy * 2 + kk) * feats, feats)

            @pl.loop(0, tokens // tile)
            def _(i):
                rows = span(self.rows(h) * tokens + i * tile, tile)
                right = self.right[cols, :] if self.dims == ((1,), (1,)) else self.right[:, cols]
                value = dot(self.left[rows, :], right, self.dims)
                self.total[rows, cols] = value.astype(jnp.bfloat16)

        def compute(self, h, yy, name):
            self.columns(h, yy, ok)
            send(
                lambda: self.tile_of(h, yy, ok),
                lambda: self.slot(h, yy),
                sid(f"{self.name}k{h}{name}"),
                at_k,
            )
            self.columns(h, yy, k)

        def far(self, h):
            self.compute(h, oy, "far")

        def near(self, h):
            self.compute(h, y, "near")

        def add(self, mine, got):
            @pl.loop(0, tokens // tile)
            def _(i):
                rows = span(i * tile, tile)
                value = mine[rows, :].astype(jnp.float32) + got[rows, :].astype(jnp.float32)
                mine[rows, :] = value.astype(jnp.bfloat16)

        def pass_on(self, way, h, yy, half):
            send(
                lambda: self.half_of(h, yy, half),
                lambda: self.half_slot(way),
                sid(self.name + way),
                at_y if way[0] == "y" else at_x,
            )

        def take(self, way, h, yy, half):
            arrived(self.half_slot(way), sid(self.name + way))
            self.add(self.half_of(h, yy, half), self.half_slot(way))

        def far_k(self, h):
            arrived(self.slot(h, oy), sid(f"{self.name}k{h}far"))
            self.add(self.tile_of(h, oy, k), self.slot(h, oy))
            self.pass_on(f"y{h + 1}", h, oy, 0 if self.both else None)
            if h == 0 and self.both:
                self.pass_on("x1", 0, oy, 1)

        def near_k(self, h):
            arrived(self.slot(h, y), sid(f"{self.name}k{h}near"))
            self.add(self.tile_of(h, y, k), self.slot(h, y))
            if h == 0 and self.both:
                self.pass_on("x2", 0, y, 1)

        def second(self):
            half = None
            if self.both:
                half = 0
                self.take("x1", 1, oy, 1)
                self.pass_on("y3", 1, oy, 1)
            self.take("y1", 0, y, half)
            self.pass_on("x3", 0, y, half)

        def finish(self):
            if self.both:
                self.take("x2", 1, y, 1)
                self.take("y3", 1, y, 1)
            half = 0 if self.both else None
            self.take("y2", 1, y, half)
            self.take("x3", 1, y, half)
            copy = pltpu.make_async_copy(
                self.tile_of(1, y, k), self.out, local_sem.at[lid(f"local {self.name}")]
            )
            copy.start()
            locals_.append(copy)

    locals_ = []
    down_sum = Sum("ds", cot_x, down_terms, down_got, down_out, down_run, 0)
    up_sum = Sum("us", earlier_x, up_terms, up_got, up_out, up_run, chunks)
    cols_of = lambda j: span(j * cw, cw)

    product = Partial("po", hidden, down_w, ((1,), (0,)), later_x, parts_got, last_got, later_out, True)
    back = Partial(
        "pb",
        gate,
        up_w,
        ((1,), (1,)),
        cot_x,
        earlier_x,
        earlier_x.at[span(0, tokens), span(3 * feats, feats)],
        grad_out,
        False,
    )
    def settle_later():
        for entry in lx.sends:
            sent(entry)

    def settle_cot():
        for entry in ct.sends:
            sent(entry)

    def settle_earlier():
        for entry in ex.sends:
            sent(entry)
        for device in (at_x, at_y, at_k):
            pl.semaphore_signal(ready_sem, inc=1, device_id=device, device_id_type=MESH)

    def others_ready():
        pl.semaphore_wait(ready_sem, 3)

    later_copies = []
    up_a[0].first()
    lx.first_k()
    ex.first_y()
    up_a[1].first()
    swap_up(0)
    swap_up(1)
    ex.first_k()
    ct.first_k()
    for copy in copies:
        copy.start()
    ex.local()
    ct.local()
    lx.local()
    swapped_up(0)
    ex.first_x()
    swapped_up(1)
    ct.first_y()
    up_b[0].inner(1)
    ct.first_x()
    down_a[1].first()
    ex.got_y()
    up_b[0].outer(1)
    ex.got_x()
    swap_down(0)
    ex.near()
    up_a[0].outer(1)
    up_a[0].inner(1)
    up_b[1].outer(1)
    up_a[1].inner(1)
    up_a[1].outer(1)
    swap_down(1)
    up_b[0].inner(2)
    ct.got_y()
    up_a[0].inner(2)
    ct.got_x()
    down_a[0].first()
    ct.near()
    ex.got_ya()
    swapped_down(0)
    up_b[0].inner(3)
    ex.whole()
    down_sum.load(0, 0)
    lx.first_y()
    up_a[0].inner(3)
    up_b[1].inner(1)
    down_a[1].outer(1)
    swapped_down(1)
    lx.first_x()
    for copy in copies:
        copy.wait()
    gate_chunk(0)
    up_a[1].inner(2)
    down_sum.compute(0, lambda: squared[...], (0, 1))
    ct.got_ya()
    ct.whole()
    down_b[0].outer(1)
    down_b[1].outer(1)
    down_sum.compute(0, lambda: squared[...], (2, 3))
    up_b[1].inner(2)
    down_sum.step(1, 0, 0)
    lx.got_x()
    lx.got_y()
    up_b[1].inner(3)
    down_sum.load(1, 1)
    up_a[1].inner(3)
    down_a[0].outer(1)
    down_b[1].inner(1)
    down_sum.load(1, 0)
    gate_chunk(1)
    down_a[1].inner(1)
    down_a[0].inner(1)
    down_b[0].inner(1)
    down_sum.compute(1, lambda: squared[...], (0, 1))
    lx.got_ya()
    lx.got_xb()
    lx.near()
    down_sum.compute(1, lambda: squared[...], (2, 3))
    lx.whole()
    down_sum.step(1, 0, 1)
    later_copies.append(later_chunk(1, squared))
    later_copies.append(later_chunk(0, staged))
    down_a[1].inner(2)
    down_b[1].inner(2)
    down_a[1].inner(3)
    down_b[0].inner(2)
    down_b[1].inner(3)
    down_a[0].inner(2)
    down_sum.step(2, 0, 0)
    down_sum.step(2, 0, 1)
    slope_chunk(1)
    down_sum.step(1, 1, 0)
    up_sum.compute(1, lambda: gate[:, cols_of(1)], range(nz))
    settle_later()
    down_a[0].inner(3)
    down_b[0].inner(3)
    down_sum.step(1, 1, 1)
    product.far(0)
    slope_chunk(0)
    down_sum.load(0, 1)
    down_sum.step(3, 0, 0)
    product.far_k(0)
    down_sum.step(2, 1, 0)
    product.far(1)
    up_sum.compute(0, lambda: gate[:, cols_of(0)], range(nz))
    settle_earlier()
    product.far_k(1)
    product.near(0)
    settle_cot()
    down_sum.step(2, 1, 1)
    others_ready()
    down_sum.step(3, 1, 0)
    down_sum.step(3, 0, 1)
    back.far(0)
    back.far_k(0)
    up_sum.step(1, 1, 0)
    back.far(1)
    product.near_k(0)
    up_sum.step(1, 1, 1)
    product.near(1)
    down_sum.own(0)
    back.near(0)
    up_sum.step(2, 1, 0)
    product.near_k(1)
    product.second()
    back.near(1)
    back.far_k(1)
    down_sum.other(1)
    down_sum.step(3, 1, 1)
    back.near_k(0)
    up_sum.step(2, 1, 1)
    up_sum.step(3, 1, 0)
    back.near_k(1)
    down_sum.other(0)
    back.second()
    up_sum.step(1, 0, 0)
    down_sum.own(1)
    up_sum.step(3, 1, 1)
    up_sum.step(1, 0, 1)
    up_sum.step(2, 0, 0)
    next_load(0, 1)
    next_load(1, 1)
    up_sum.step(2, 0, 1)
    up_sum.step(3, 0, 0)
    next_load(0, 0)
    product.finish()
    up_sum.step(3, 0, 1)
    up_sum.own(1)
    up_sum.own(0)
    up_sum.other(1)
    next_load(1, 0)
    back.finish()
    up_sum.other(0)
    for j in range(chunks):
        arrived(preact_out.at[:, span(ox * width + j * cw, cw)], sid(f"pre{j}"))
    for copy in later_copies + locals_ + list(up_sum.stores.values()):
        copy.wait()
    for entry in pending:
        sent(entry)


def on_device_rings(
    later_input, earlier_input, cotangent, up_weight, down_weight, up_running, down_running
):
    n = lax.axis_size("fs")
    factor = float(later_input.shape[0] * n) ** (-0.5)

    up_full, up_arrived = ring_gather(up_weight)
    inputs = tp_gather(jnp.stack((later_input, earlier_input, cotangent)))
    later_full, earlier_full, cot_full = inputs[0], inputs[1], inputs[2]
    down_rows = after(down_weight.T, inputs, *up_arrived[-4])
    down_full, down_arrived = ring_gather(down_rows)

    earlier_up = jnp.dot(earlier_full, up_full, preferred_element_type=jnp.float32)
    earlier_relu = jax.nn.relu(earlier_up)
    earlier_hidden = jnp.square(earlier_relu).astype(jnp.bfloat16)
    down_terms = lax.dot_general(
        cot_full, earlier_hidden, contract_first, preferred_element_type=jnp.float32
    ).astype(jnp.bfloat16)
    down_sum = ring_scatter(down_terms, down_arrived[-4])

    later_up = jnp.dot(later_full, up_full, preferred_element_type=jnp.float32)
    later_preact = later_up.astype(jnp.bfloat16)
    later_hidden = jnp.square(jax.nn.relu(later_up)).astype(jnp.bfloat16)

    grad = jnp.dot(cot_full, down_full, preferred_element_type=jnp.float32)
    up_grad = (2.0 * earlier_relu * grad).astype(jnp.bfloat16)
    up_terms = lax.dot_general(
        earlier_full, up_grad, contract_first, preferred_element_type=jnp.float32
    ).astype(jnp.bfloat16)
    up_sum = ring_scatter(up_terms)

    back_part = lax.dot_general(
        up_grad, up_full, contract_last, preferred_element_type=jnp.float32
    ).astype(jnp.bfloat16)
    product = lax.dot_general(
        later_hidden, down_full, contract_last, preferred_element_type=jnp.float32
    ).astype(jnp.bfloat16)
    return (
        tp_scatter(product),
        later_preact,
        tp_scatter(back_part),
        up_running + up_sum * factor,
        down_running + down_sum * factor,
    )


def across_x(n_fs):
    return 1 << ((n_fs.bit_length() - 1) // 2)


def hand_over_kernel(pieces, count, *refs):
    sources, targets, held = refs[:count], refs[count : 2 * count], refs[2 * count : 3 * count]
    in_sem, out_sem = refs[3 * count :]
    reads, writes = [], []
    for n, rows, size in pieces:
        part, index = pl.ds(rows, size), len(reads)
        here = held[n].at[part, :]
        reads.append(pltpu.make_async_copy(sources[n].at[part, :], here, in_sem.at[index]))
        writes.append(pltpu.make_async_copy(here, targets[n].at[part, :], out_sem.at[index]))
    for read in reads:
        read.start()
    for read, write in zip(reads, writes):
        read.wait()
        write.start()
    for write in writes:
        write.wait()


def hand_over(arrays):
    pieces = []
    for n, array in enumerate(arrays):
        size = max(array.shape[0] * MIB // (array.size * array.dtype.itemsize), 1)
        size = math.gcd(array.shape[0], 1 << (size.bit_length() - 1))
        pieces += [(n, rows, size) for rows in range(0, array.shape[0], size)]
    in_hbm = pl.BlockSpec(memory_space=pltpu.HBM)
    return pl.pallas_call(
        functools.partial(hand_over_kernel, pieces, len(arrays)),
        out_shape=tuple(jax.ShapeDtypeStruct(a.shape, a.dtype) for a in arrays),
        in_specs=[in_hbm] * len(arrays),
        out_specs=(in_hbm,) * len(arrays),
        scratch_shapes=[pltpu.VMEM(a.shape, a.dtype) for a in arrays]
        + [pltpu.SemaphoreType.DMA((len(pieces),))] * 2,
        compiler_params=pltpu.CompilerParams(vmem_limit_bytes=VMEM_BYTES),
        name="hand_over",
    )(*arrays)


def on_device_kernel(
    later_input, earlier_input, cotangent, up_weight, down_weight, up_running, down_running
):
    n = lax.axis_size("fs")
    nz = n // 2
    tokens, feats = later_input.shape
    fan, width = up_weight.shape[0], up_weight.shape[1] // 2
    depth, rows = n * fan, 2 * tokens
    factor = float(tokens * n) ** (-0.5)
    bf16 = jnp.bfloat16
    semaphores = 32 * (nz - 1) + 50
    anywhere = pl.BlockSpec(memory_space=pl.ANY)
    outputs = pl.pallas_call(
        functools.partial(layer_kernel, nz, factor),
        out_shape=(
            jax.ShapeDtypeStruct((tokens, feats), bf16),
            jax.ShapeDtypeStruct((tokens, 2 * width), bf16),
            jax.ShapeDtypeStruct((tokens, feats), bf16),
            jax.ShapeDtypeStruct((fan, 2 * width), jnp.float32),
            jax.ShapeDtypeStruct((fan, 2 * width), jnp.float32),
        ),
        in_specs=[anywhere] * 7,
        out_specs=(anywhere,) * 5,
        scratch_shapes=[
            pltpu.VMEM((rows, depth), bf16),
            pltpu.VMEM((rows, depth), bf16),
            pltpu.VMEM((rows, depth), bf16),
            pltpu.VMEM((depth, width), bf16),
            pltpu.VMEM((width, depth), bf16),
            pltpu.VMEM((rows, width), bf16),
            pltpu.VMEM((rows, width), bf16),
            pltpu.VMEM((rows, width // 2), bf16),
            pltpu.VMEM((rows, width // 2), bf16),
            pltpu.VMEM((depth, width), bf16),
            pltpu.VMEM((depth, width), bf16),
            pltpu.VMEM((nz + 1, 2 * fan, width), bf16),
            pltpu.VMEM((nz + 1, 2 * fan, width), bf16),
            pltpu.VMEM((rows, 3 * feats), bf16),
            pltpu.VMEM((tokens, feats), bf16),
            pltpu.VMEM((4, fan, width // 2), bf16),
            pltpu.VMEM((4, fan, width // 2), jnp.float32),
            pltpu.SemaphoreType.DMA((semaphores,)),
            pltpu.SemaphoreType.DMA((semaphores,)),
            pltpu.SemaphoreType.DMA((27,)),
            pltpu.SemaphoreType.REGULAR,
        ],
        compiler_params=pltpu.CompilerParams(
            collective_id=0, has_side_effects=True, vmem_limit_bytes=VMEM_BYTES
        ),
        name="layer",
    )(later_input, earlier_input, cotangent, up_weight, down_weight, up_running, down_running)
    return hand_over(outputs)


def on_device(*arrays):
    square = across_x(lax.axis_size("fs")) == 2 and lax.axis_size("tp") == 4
    return (on_device_kernel if square else on_device_rings)(*arrays)


def solution(mesh):
    in_specs = (
        P("fs", "tp"),
        P("fs", "tp"),
        P("fs", "tp"),
        P("fs", "tp"),
        P("tp", "fs"),
        P("fs", "tp"),
        P("fs", "tp"),
    )
    out_specs = (P("fs", "tp"), P("fs", "tp"), P("fs", "tp"), P("fs", "tp"), P("fs", "tp"))
    return jax.shard_map(
        on_device, mesh=mesh, in_specs=in_specs, out_specs=out_specs, check_vma=False
    )
```
